32 devices in a mesh: ep: 16 (over z, x, core), tp: 2 (over y).
Axes of the slice: x: 2, y: 2, z: 4, core: 2. Of those that a mesh axis runs over, the one named last changes fastest.
Arguments:
- tokens: bfloat16 [2048, 2048], P('ep'), may hold values from -6 to 6
- cotangent: bfloat16 [2048, 2048], P('ep'), may hold values from -1.796875 to 1.796875
- group_weight: float32 [2048], P('ep'), may hold values from 0.2 to 1
- expert_weight: float32 [2048, 2], P('ep'), may hold values from 0.1 to 0.9
- group_choice: int32 [2048], P('ep'), may hold values from 0 to 3, as said below
- local_choice: int32 [2048, 2], P('ep'), may hold values from 0 to 3, as said below
- w_gate: bfloat16 [16, 2048, 512], P('ep', None, 'tp'), may hold values from -0.125 to 0.125
- w_up: bfloat16 [16, 2048, 512], P('ep', None, 'tp'), may hold values from -0.125 to 0.125
- w_down: bfloat16 [16, 512, 2048], P('ep', 'tp'), may hold values from -0.25 to 0.25
Outputs:
- token_grad: float32 [2048, 2048], P('ep', 'tp')
- group_weight_grad: float32 [2048], P('ep')
- expert_weight_grad: float32 [2048, 2], P('ep')
- w_gate_grad: float32 [16, 2048, 512], P('ep', None, 'tp')
- w_up_grad: float32 [16, 2048, 512], P('ep', None, 'tp')
- w_down_grad: float32 [16, 512, 2048], P('ep', 'tp')
The draws below stay inside these ranges and needn't reach their ends.
Inputs may be any that keep to these rules, and one draw needn't show every extreme that they name: Among the 128 tokens of each device (aligned blocks of tokens), no expert 4 * group_choice + local_choice is named by more than 24 slots, and some expert is named by exactly 24 slots of every device. `local_choice`: the 2 local choices of a token differ.
All inputs are finite; a program needn't handle non-finite values.
Results may differ from the reference program's by a relative error of at most 0.006.
Values may be sent and summed in bfloat16 or wider, within the bound.
A program may use at most 64 MiB of HBM per device.

```python
import math
import jax
import jax.numpy as jnp
from jax import lax

D = 2048
F = 512
EPG = 4
TOP_K = 2
TOK_DEV = 128
TOKENS = 2048
EXPERTS = 16
GROUPS = 4
CAP = 24
N_EP = 16


def route_tables(key):
    folded = jax.random.fold_in(key, 11)
    key_hot, key_perm, key_order, key_shift, key_step = jax.random.split(folded, 5)
    block_count = TOKENS // TOK_DEV
    busiest = EPG * CAP // TOP_K
    hot_group = jax.random.randint(key_hot, (), 0, GROUPS, dtype=jnp.int32)
    arrange = jax.vmap(lambda member_key: jax.random.permutation(member_key, TOK_DEV))(jax.random.split(key_perm, block_count)).astype(jnp.int32)
    others = jax.vmap(lambda member_key: jax.random.permutation(member_key, GROUPS - 1))(jax.random.split(key_order, block_count)).astype(jnp.int32)
    places = jnp.arange(TOK_DEV, dtype=jnp.int32)
    beyond = jnp.maximum(places - busiest, 0)
    column_ids = jnp.broadcast_to(beyond % (GROUPS - 1), (block_count, TOK_DEV))
    other_pick = jnp.take_along_axis(others, column_ids, axis=1)
    other_group = other_pick + (other_pick >= hot_group).astype(jnp.int32)
    group_at = jnp.where(places[None, :] < busiest, hot_group, other_group)
    rank_at = jnp.where(places < busiest, places, beyond // (GROUPS - 1))[None, :]
    shifts = jax.random.randint(key_shift, (block_count, GROUPS), 0, EPG, dtype=jnp.int32)
    strides = jax.random.randint(key_step, (block_count, GROUPS), 1, EPG, dtype=jnp.int32)
    first_local = (rank_at + jnp.take_along_axis(shifts, group_at, axis=1)) % EPG
    stride_at = jnp.take_along_axis(strides, group_at, axis=1)
    local_at = (first_local[..., None] + jnp.arange(TOP_K, dtype=jnp.int32) * stride_at[..., None]) % EPG
    inverse = jnp.argsort(arrange, axis=1, stable=True).astype(jnp.int32)
    group_table = jnp.take_along_axis(group_at, inverse, axis=1)
    local_table = jnp.take_along_axis(local_at, inverse[..., None], axis=1)
    return (group_table.reshape(TOKENS).astype(jnp.int32), local_table.reshape(TOKENS, TOP_K).astype(jnp.int32))


def draw_group_choice(key, part):
    return route_tables(key)[0]


def draw_local_choice(key, part):
    return route_tables(key)[1]


def level_of(own_key, extent, cuts, smallest, high):
    level = 1.0
    for dim, shards_of in cuts:
        draws = jax.random.uniform(jax.random.fold_in(jax.random.fold_in(own_key, 6), dim), (shards_of,), jnp.float32, smallest / len(cuts), high / len(cuts))
        level = level * jnp.repeat(jnp.exp(draws), extent[dim] // shards_of).reshape((-1,) + (1,) * (len(extent) - 1 - dim))
    return level


def noise(own_key, dims, scale, bound, cuts=(), kind=jnp.bfloat16):
    values = jax.random.normal(own_key, dims, jnp.float32) * scale
    if len(cuts) > 0:
        values = level_of(own_key, dims, cuts, -0.22, 0.18) * values
    return jnp.clip(values, min=-bound, max=bound).astype(kind)


def setup_inputs(seed: int = 0) -> dict:
    keys = jax.random.split(jax.random.key(seed), 10)
    return {
        "tokens": noise(keys[0], (TOKENS, D), 1.0, 6.0, ((0, 16),)),
        "cotangent": noise(keys[1], (TOKENS, D), 0.3, 1.796875, ((0, 16),)),
        "group_weight": jnp.clip(jnp.exp(math.log(1.0) - 1.609438 * jax.random.uniform(keys[2], (TOKENS,), jnp.float32) ** level_of(keys[2], (TOKENS,), ((0, 16),), -0.2, 0.2)), 0.2, 1.0),
        "expert_weight": jnp.clip(0.1 + 0.79999997 * jax.random.uniform(keys[3], (TOKENS, TOP_K), jnp.float32) ** level_of(keys[3], (TOKENS, TOP_K), ((0, 16),), -0.2, 0.2), 0.1, 0.9),
        "group_choice": draw_group_choice(jax.random.fold_in(keys[9], 71), 0),
        "local_choice": draw_local_choice(jax.random.fold_in(keys[9], 71), 0),
        "w_gate": noise(keys[6], (EXPERTS, D, F), D ** -0.5, 0.125, ((0, 16), (2, 2))),
        "w_up": noise(keys[7], (EXPERTS, D, F), D ** -0.5, 0.125, ((0, 16), (2, 2))),
        "w_down": noise(keys[8], (EXPERTS, F, D), F ** -0.5, 0.25, ((0, 16), (1, 2))),
    }


def expert_backward(arrived, cot_rows, gate_rows, first, second, third):
    pre_gate = jnp.dot(arrived, first, preferred_element_type=jnp.float32)
    pre_up = jnp.dot(arrived, second, preferred_element_type=jnp.float32)
    back_hidden = jnp.dot(cot_rows, third.T, preferred_element_type=jnp.float32)
    sigma = jax.nn.sigmoid(pre_gate)
    swish = pre_gate * sigma
    hidden = swish * pre_up
    gate_part = jnp.sum(hidden * back_hidden, axis=1)
    gate_float = gate_rows.astype(jnp.float32)[:, None]
    scaled = gate_float * back_hidden
    grad_gate_pre = (scaled * pre_up * sigma * (1.0 + pre_gate * (1.0 - sigma))).astype(jnp.bfloat16)
    grad_up_pre = (scaled * swish).astype(jnp.bfloat16)
    weighted = (gate_float * hidden).astype(jnp.bfloat16)
    first_grad = jnp.dot(arrived.T, grad_gate_pre, preferred_element_type=jnp.float32)
    second_grad = jnp.dot(arrived.T, grad_up_pre, preferred_element_type=jnp.float32)
    third_grad = jnp.dot(weighted.T, cot_rows, preferred_element_type=jnp.float32)
    total = jnp.dot(grad_gate_pre, first.T, preferred_element_type=jnp.float32)
    total = total + jnp.dot(grad_up_pre, second.T, preferred_element_type=jnp.float32)
    row_grad = total.astype(jnp.bfloat16)
    return first_grad, second_grad, third_grad, row_grad, gate_part


def reference(tokens, cotangent, group_weight, expert_weight, group_choice, local_choice, w_gate, w_up, w_down):
    slot_total = TOKENS * TOP_K
    expert_of = (group_choice[:, None] * EPG + local_choice).reshape(slot_total).astype(jnp.int32)
    member = (expert_of[:, None] == jnp.arange(EXPERTS, dtype=jnp.int32)[None, :]).astype(jnp.int32)
    running = jnp.cumsum(member, axis=0).astype(jnp.int32) - 1
    position = jnp.sum(running * member, axis=1).astype(jnp.int32)
    buffer_rows = N_EP * CAP
    slot_ids = jnp.arange(slot_total, dtype=jnp.int32)
    owner = jnp.full((EXPERTS, buffer_rows), slot_total, jnp.int32).at[expert_of, position].set(slot_ids)
    gate_value = (group_weight[:, None] * expert_weight).astype(jnp.bfloat16).reshape(slot_total)

    def per_expert(index):
        chosen = owner[index]
        live = chosen < slot_total
        safe = jnp.minimum(chosen, slot_total - 1)
        token_ids = (safe // TOP_K).astype(jnp.int32)
        zero = jnp.zeros((), jnp.bfloat16)
        arrived = jnp.where(live[:, None], tokens[token_ids], zero)
        cot_rows = jnp.where(live[:, None], cotangent[token_ids], zero)
        gate_rows = jnp.where(live, gate_value[safe], zero)
        return expert_backward(arrived, cot_rows, gate_rows, w_gate[index], w_up[index], w_down[index])

    first_grad, second_grad, third_grad, row_grad, gate_part = lax.map(per_expert, jnp.arange(EXPERTS, dtype=jnp.int32))
    slot_grad = row_grad[expert_of, position].astype(jnp.float32)
    token_grad = jnp.sum(slot_grad.reshape(TOKENS, TOP_K, D), axis=1)
    held = lax.optimization_barrier(gate_part[expert_of, position].astype(jnp.bfloat16))
    gate_grad = held.astype(jnp.float32).reshape(TOKENS, TOP_K)
    group_grad = jnp.sum(expert_weight * gate_grad, axis=1)
    expert_grad = group_weight[:, None] * gate_grad
    return (token_grad, group_grad, expert_grad, first_grad, second_grad, third_grad)
```

```python
import functools

import jax
import jax.numpy as jnp
from jax import lax
from jax.experimental import pallas as pl
from jax.experimental.pallas import tpu as pltpu
from jax.sharding import Mesh, PartitionSpec as P

EPG = 4
LANES = 128

MESH = pl.DeviceIdType.MESH

CONTRACT_COLS = (((1,), (1,)), ((), ()))
CONTRACT_ROWS = (((0,), (0,)), ((), ()))


def partner(g, d, groups, sign):
    if groups & (groups - 1):
        return lax.rem(g + sign * d + groups, groups)
    met, bit = g, 1
    while bit < groups:
        if d & bit:
            met = met + bit - 2 * bit * ((g // bit) % 2)
        bit *= 2
    return met


class Copies:
    def __init__(self, send_sem, recv_sem):
        self.send_sem, self.recv_sem, self.made = send_sem, recv_sem, []

    def start(self, src, dst, device):
        number = len(self.made)
        copy = pltpu.make_async_remote_copy(
            src_ref=src,
            dst_ref=dst,
            send_sem=self.send_sem.at[number],
            recv_sem=self.recv_sem.at[number],
            device_id=device,
            device_id_type=MESH,
        )
        copy.start()
        self.made.append(copy)
        return copy

    def finish(self):
        for copy in self.made:
            copy.wait_send()


def copy_count(groups, lanes):
    far = lanes - 1
    first = (groups - 1) * 3
    spread = (groups - 1) * (2 + 4 * far) + 2 + 2 * far
    inside = groups * 7
    back = groups * (4 + 2 * far) + groups - 1
    return first + spread + inside + back


def dot(a, b):
    return jnp.dot(a, b, preferred_element_type=jnp.float32)


def add(*parts):
    total = parts[0].astype(jnp.float32)
    for part in parts[1:]:
        total = total + part.astype(jnp.float32)
    return total.astype(jnp.bfloat16)


def plan(groups):
    steps = []
    later = list(range(1, groups))
    steps += [("own", 0), ("arrive", later[0]) if later else ("none", 0), ("relay", 0)]
    for d in later:
        if d > 1:
            steps.append(("arrive", d))
        steps.append(("relay", d))
        steps.append(("inside", d - 1))
        steps.append(("compute", d - 1))
        if d >= 3:
            steps.append(("sum_cores", d - 2))
    last = groups - 1
    steps += [("inside", last), ("compute", last)]
    order = later + [0]
    started = {d for name, d in steps if name == "sum_cores"}
    queue = [d for d in order if d not in started]
    running = [d for d in order if d in started]
    steps += [("sum_cores", d) for d in queue[:1]]
    done = []
    stage = {d: 1 for d in running + queue[:1]}
    waiting = queue[1:]
    while stage or waiting:
        if waiting:
            d = waiting.pop(0)
            steps.append(("sum_cores", d))
            stage[d] = 1
        steps.append(("weights", 0))
        for d in [d for d in order if stage.get(d) == 2][:1]:
            steps.append(("last_sum", d))
            del stage[d]
        for d in [d for d in order if stage.get(d) == 1][:1]:
            steps.append(("middle_sum", d))
            stage[d] = 2
    steps.append(("weights_end", 0))
    return steps


def kernel(
    groups, lanes, cap, wide0, wide1,
    pick, gate_cols, tokens, cotangent, w_gate, w_up, w_down,
    result, grad_first, grad_second, grad_third,
    out_t, out_c, out_g, tok, cot, gate, first, second, third,
    gg, gu, wt, wt_t, part_a, part_b, rc_a, rc_b, s1_a, s1_b, rx_a, rl_a, rl_b, s2_a, s2_b, rx_b,
    done, ret, send, recv, loc,
):
    g, e, y = lax.axis_index("g"), lax.axis_index("e"), lax.axis_index("tp")
    x, c = e // 2, e % 2
    ex, ec = (g, (1 - x) * 2 + c, y), (g, x * 2 + (1 - c), y)
    token_count, feature_count = tokens.shape
    piece = feature_count // lanes
    hidden_count = gg.shape[1]
    rows = EPG * cap
    far = range(1, lanes)
    ahead = [lax.rem(y + r, lanes) for r in far]
    behind = [lax.rem(y + lanes - r, lanes) for r in far]
    others = [(g, e, lane) for lane in ahead]

    barrier = pltpu.get_barrier_semaphore()
    met = [(lax.rem(g + d, groups), e, y) for d in range(1, groups)] + others + [ex, ec]
    for device in met:
        pl.semaphore_signal(barrier, inc=1, device_id=device, device_id_type=MESH)
    loads = [
        pltpu.make_async_copy(src, dst, loc.at[i])
        for i, (src, dst) in enumerate(((w_gate, first), (w_up, second), (w_down, third)))
    ]
    for load in loads:
        load.start()

    chosen = pick[...].reshape(groups * cap, token_count)
    columns = pl.ds(pl.multiple_of(y * piece, LANES), piece)

    def spread_rows(rows_of, source):
        return dot(rows_of, source).astype(jnp.bfloat16)

    out_t[...] = spread_rows(chosen, tokens[:, columns]).reshape(groups, cap, piece)
    out_c[...] = spread_rows(chosen, cotangent[:, columns]).reshape(groups, cap, piece)
    out_g[...] = spread_rows(chosen, gate_cols[...]).reshape(groups, cap, LANES)
    pl.semaphore_wait(barrier, len(met))

    copies = Copies(send, recv)
    state = [dict() for _ in range(groups)]
    for d in range(1, groups):
        target = partner(g, d, groups, -1)
        there = (target, e, y)
        state[d]["zt"] = copies.start(out_t.at[target], tok.at[y, d, 0], there)
        state[d]["zg"] = copies.start(out_g.at[target], gate.at[d, 0], there)
        state[d]["zc"] = copies.start(out_c.at[target], cot.at[y, d, 0], there)

    def own(_):
        s = state[0]
        s["tx"] = [copies.start(out_t.at[g], tok.at[y, 0, 1], ex)]
        s["gx"] = copies.start(out_g.at[g], gate.at[0, 1], ex)
        s["cx"] = copies.start(out_c.at[g], cot.at[y, 0, 1], ex)
        mine = pick[g]
        for lane in range(lanes):
            cols = slice(lane * piece, (lane + 1) * piece)
            tok[lane, 0, 0] = spread_rows(mine, tokens[:, cols])
            cot[lane, 0, 0] = spread_rows(mine, cotangent[:, cols])
        gate[0, 0] = out_g[g]
        s["core"] = [
            copies.start(out_g.at[g], gate.at[0, 2], ec),
            copies.start(tok.at[:, 0, 0], tok.at[:, 0, 2], ec),
            copies.start(cot.at[:, 0, 0], cot.at[:, 0, 2], ec),
        ]

    def arrive(d):
        s = state[d]
        s["zt"].wait_recv()
        mine = tok.at[y, d, 0]
        s["tl"] = [copies.start(mine, mine, device) for device in others]
        s["tx"] = [copies.start(mine, tok.at[y, d, 1], ex)]
        s["zg"].wait_recv()
        s["gx"] = copies.start(gate.at[d, 0], gate.at[d, 1], ex)
        s["core"] = [copies.start(gate.at[d, 0], gate.at[d, 2], ec)]
        s["zc"].wait_recv()
        mine = cot.at[y, d, 0]
        s["cx"] = [copies.start(mine, cot.at[y, d, 1], ex)][0]
        s["cl"] = [copies.start(mine, mine, device) for device in others]

    def relay(d):
        s = state[d]
        if d == 0:
            s["tx"][0].wait_recv()
            theirs = tok.at[y, 0, 1]
            s["txl"] = [copies.start(theirs, theirs, device) for device in others]
        else:
            for i, copy in enumerate(s["tl"]):
                copy.wait_recv()
                theirs = tok.at[behind[i], d, 0]
                s["tx"].append(copies.start(theirs, tok.at[behind[i], d, 1], ex))
            s["core"].append(copies.start(tok.at[:, d, 0], tok.at[:, d, 2], ec))
        s["cx"].wait_recv()
        theirs = cot.at[y, d, 1]
        s["cxl"] = [copies.start(theirs, theirs, device) for device in others]

    def inside(d):
        s = state[d]
        if d == 0:
            for copy in s["txl"]:
                copy.wait_recv()
        else:
            for copy in s["cl"]:
                copy.wait_recv()
            s["core"].append(copies.start(cot.at[:, d, 0], cot.at[:, d, 2], ec))
            for copy in s["tx"]:
                copy.wait_recv()
        s["core"].append(copies.start(tok.at[:, d, 1], tok.at[:, d, 3], ec))
        s["gx"].wait_recv()
        s["core"].append(copies.start(gate.at[d, 1], gate.at[d, 3], ec))
        for copy in s["cxl"]:
            copy.wait_recv()
        s["core"].append(copies.start(cot.at[:, d, 1], cot.at[:, d, 3], ec))

    loaded = []

    def compute(d):
        s = state[d]
        if not loaded:
            for load in loads:
                load.wait()
            loaded.append(True)
        for copy in s["core"]:
            copy.wait_recv()
        pre_gate = pre_up = back = None
        for lane in range(lanes):
            cols = slice(lane * piece, (lane + 1) * piece)
            rows_t = tok[lane, d].reshape(rows, piece)
            rows_c = cot[lane, d].reshape(rows, piece)
            one = dot(rows_t, first[cols, :])
            two = dot(rows_t, second[cols, :])
            three = lax.dot_general(
                rows_c, third[:, cols], CONTRACT_COLS, preferred_element_type=jnp.float32
            )
            pre_gate = one if lane == 0 else pre_gate + one
            pre_up = two if lane == 0 else pre_up + two
            back = three if lane == 0 else back + three
        own_col = lax.broadcasted_iota(jnp.int32, (rows, LANES), 1) == e
        gates = gate[d].reshape(rows, LANES).astype(jnp.float32)
        gate_float = jnp.sum(jnp.where(own_col, gates, 0.0), axis=1, keepdims=True)
        sigma = jax.nn.sigmoid(pre_gate)
        swish = pre_gate * sigma
        hidden = swish * pre_up
        gate_part = jnp.sum(hidden * back, axis=1, keepdims=True)
        scaled = gate_float * back
        grad_gate = (scaled * pre_up * sigma * (1.0 + pre_gate * (1.0 - sigma))).astype(jnp.bfloat16)
        grad_up = (scaled * swish).astype(jnp.bfloat16)
        at = slice(d * rows, (d + 1) * rows)
        gg[at, :] = grad_gate
        gu[at, :] = grad_up
        wt[at, :] = (gate_float * hidden).astype(jnp.bfloat16)
        gate_out = jnp.where(own_col, gate_part, 0.0).astype(jnp.bfloat16)

        def rows_back(lo, hi):
            total = lax.dot_general(
                grad_gate, first[lo:hi, :], CONTRACT_COLS, preferred_element_type=jnp.float32
            ) + lax.dot_general(
                grad_up, second[lo:hi, :], CONTRACT_COLS, preferred_element_type=jnp.float32
            )
            return total.astype(jnp.bfloat16).reshape(EPG, cap, hi - lo)

        for lane in range(lanes):
            lo = lane * piece
            part_a[d, lane] = rows_back(lo, lo + wide0)
            if wide0 < piece:
                part_b[d, lane, :, :, : piece - wide0] = rows_back(lo + wide0, lo + piece)
            part_b[d, lane, :, :, piece - wide0 :] = gate_out.reshape(EPG, cap, LANES)
        s["pa"] = copies.start(part_a.at[d, :, pl.ds(2, 2)], rc_a.at[d], ec)
        s["pb"] = copies.start(part_b.at[d, :, pl.ds(2, 2)], rc_b.at[d], ec)

    def sum_cores(d):
        s = state[d]
        s["pa"].wait_recv()
        s1_a[d] = add(part_a[d, :, 0:2], rc_a[d])
        s["x0"] = copies.start(s1_a.at[d, :, 1], rx_a.at[d], ex)
        s["pb"].wait_recv()
        s1_b[d] = add(part_b[d, :, 0:2], rc_b[d])
        s["l1"] = [
            copies.start(s1_b.at[d, lane], rl_b.at[d, i], (g, e, lane))
            for i, lane in enumerate(ahead)
        ]

    def middle_sum(d):
        s = state[d]
        s["x0"].wait_recv()
        s2_a[d] = add(s1_a[d, :, 0], rx_a[d])
        s["l0"] = [
            copies.start(s2_a.at[d, lane], rl_a.at[d, i], (g, e, lane))
            for i, lane in enumerate(ahead)
        ]
        for copy in s["l1"]:
            copy.wait_recv()
        s2_b[d] = add(s1_b[d, y], *[rl_b[d, i] for i in range(lanes - 1)])
        s["x1"] = copies.start(s2_b.at[d, 1], rx_b.at[d], ex)

    def last_sum(d):
        s = state[d]
        for copy in s["l0"]:
            copy.wait_recv()
        head = add(s2_a[d, y], *[rl_a[d, i] for i in range(lanes - 1)])
        s["x1"].wait_recv()
        tail = add(s2_b[d, 0], rx_b[d])
        if d == 0:
            ret[g, :, :wide0] = head
            ret[g, :, wide0:] = tail
        else:
            done[d, :, :wide0] = head
            done[d, :, wide0:] = tail
            there = (partner(g, d, groups, 1), e, y)
            s["z"] = copies.start(done.at[d], ret.at[g], there)

    tile = min(2 * LANES, piece)
    per = piece // tile
    tiles = feature_count // tile
    seen = [0]

    def weights_to(end):
        if seen[0] == 0 and end > 0:
            wt_t[...] = wt[...].T
        grads_gate, grads_up = gg[...], gu[...]
        left = wt_t[...]

        def turn(i, carry):
            lane, cols = i // per, pl.ds(pl.multiple_of(lax.rem(i, per) * tile, LANES), tile)
            turned = tok[lane, :, :, :, cols].reshape(groups * rows, tile).T
            at = pl.ds(pl.multiple_of(i * tile, LANES), tile)
            grad_first[at, :] = dot(turned, grads_gate)
            grad_second[at, :] = dot(turned, grads_up)
            grad_third[:, at] = dot(left, cot[lane, :, :, :, cols].reshape(groups * rows, tile))
            return carry

        if end > seen[0]:
            lax.fori_loop(seen[0], end, turn, 0)
        seen[0] = end

    steps = plan(groups)
    shares = sum(name == "weights" for name, _ in steps)
    served = [0]

    def weights(_):
        served[0] += 1
        weights_to(tiles * served[0] // shares)

    def weights_end(_):
        weights_to(tiles)

    phases = {
        "own": own, "arrive": arrive, "relay": relay, "inside": inside, "compute": compute,
        "sum_cores": sum_cores, "middle_sum": middle_sum, "last_sum": last_sum,
        "weights": weights, "weights_end": weights_end,
    }
    for name, d in steps:
        if name in phases:
            phases[name](d)
    for d in range(1, groups):
        state[d]["z"].wait_recv()
    result[...] = lax.dot_general(
        chosen,
        ret[...].reshape(groups * cap, wide0 + wide1),
        CONTRACT_ROWS,
        preferred_element_type=jnp.float32,
    )
    copies.finish()


def route(pick, gate_cols, tokens, cotangent, w_gate, w_up, w_down, groups, lanes, cap):
    token_count, feature_count = tokens.shape
    hidden_count = w_gate.shape[1]
    piece = feature_count // lanes
    wide1 = (piece + LANES) // (2 * LANES) * LANES
    wide0 = piece + LANES - wide1
    rows = EPG * cap
    far = max(lanes - 1, 1)
    count = copy_count(groups, lanes)
    vmem, hbm = pl.BlockSpec(memory_space=pltpu.VMEM), pl.BlockSpec(memory_space=pl.ANY)

    def buffer(*shape):
        return pltpu.VMEM(shape, jnp.bfloat16)

    def grad(*shape):
        return jax.ShapeDtypeStruct(shape, jnp.float32)

    return pl.pallas_call(
        functools.partial(kernel, groups, lanes, cap, wide0, wide1),
        out_shape=(
            grad(token_count, wide0 + wide1),
            grad(feature_count, hidden_count),
            grad(feature_count, hidden_count),
            grad(hidden_count, feature_count),
        ),
        in_specs=[vmem] * 4 + [hbm] * 3,
        out_specs=(vmem,) * 4,
        scratch_shapes=[
            buffer(groups, cap, piece),
            buffer(groups, cap, piece),
            buffer(groups, cap, LANES),
            buffer(lanes, groups, EPG, cap, piece),
            buffer(lanes, groups, EPG, cap, piece),
            buffer(groups, EPG, cap, LANES),
            buffer(feature_count, hidden_count),
            buffer(feature_count, hidden_count),
            buffer(hidden_count, feature_count),
            buffer(groups * rows, hidden_count),
            buffer(groups * rows, hidden_count),
            buffer(groups * rows, hidden_count),
            buffer(hidden_count, groups * rows),
            buffer(groups, lanes, EPG, cap, wide0),
            buffer(groups, lanes, EPG, cap, wide1),
            buffer(groups, lanes, 2, cap, wide0),
            buffer(groups, lanes, 2, cap, wide1),
            buffer(groups, lanes, 2, cap, wide0),
            buffer(groups, lanes, 2, cap, wide1),
            buffer(groups, lanes, cap, wide0),
            buffer(groups, far, cap, wide0),
            buffer(groups, far, 2, cap, wide1),
            buffer(groups, lanes, cap, wide0),
            buffer(groups, 2, cap, wide1),
            buffer(groups, cap, wide1),
            buffer(groups, cap, wide0 + wide1),
            buffer(groups, cap, wide0 + wide1),
            pltpu.SemaphoreType.DMA((count,)),
            pltpu.SemaphoreType.DMA((count,)),
            pltpu.SemaphoreType.DMA((3,)),
        ],
        compiler_params=pltpu.CompilerParams(
            collective_id=0, has_side_effects=True, vmem_limit_bytes=60 * 1024 * 1024
        ),
        name="routed_backward",
    )(pick, gate_cols, tokens, cotangent, w_gate, w_up, w_down)


def shards(
    tokens, cotangent, group_weight, expert_weight, group_choice, local_choice, w_gate, w_up, w_down
):
    token_count, feature_count = tokens.shape
    pick_count = expert_weight.shape[1]
    group_count = lax.axis_size("g")
    lane_count = lax.axis_size("tp")
    expert_count = group_count * EPG
    capacity = pick_count * (3 * token_count // (2 * expert_count))
    group_cap = -(-(EPG * capacity // pick_count) // 16) * 16
    row_count = group_count * group_cap
    piece = feature_count // lane_count
    order = jnp.arange(token_count, dtype=jnp.int32)
    same = (group_choice[:, None] == group_choice[None, :]) & (order[:, None] > order[None, :])
    dest = group_choice * group_cap + jnp.sum(same.astype(jnp.int32), axis=1)
    pick = (jnp.arange(row_count, dtype=jnp.int32)[:, None] == dest[None, :]).astype(jnp.bfloat16)
    gate = (group_weight[:, None] * expert_weight).astype(jnp.bfloat16)
    named = local_choice[:, :, None] == jnp.arange(LANES, dtype=jnp.int32)
    gate_cols = jnp.sum(jnp.where(named, gate[:, :, None], 0), axis=1).astype(jnp.bfloat16)
    result, first_grad, second_grad, third_grad = route(
        pick.reshape(group_count, group_cap, token_count),
        gate_cols,
        tokens,
        cotangent,
        w_gate[0],
        w_up[0],
        w_down[0],
        group_count,
        lane_count,
        group_cap,
    )
    token_grad = result[:, :piece]
    gate_grad = jnp.sum(jnp.where(named, result[:, None, piece:], 0.0), axis=2)
    gate_grad = gate_grad.astype(jnp.bfloat16).astype(jnp.float32)
    group_grad = jnp.sum(expert_weight * gate_grad, axis=1)
    expert_grad = group_weight[:, None] * gate_grad
    return (
        token_grad,
        group_grad,
        expert_grad,
        first_grad[None],
        second_grad[None],
        third_grad[None],
    )


def solution(mesh):
    lanes = mesh.shape["tp"]
    split = Mesh(mesh.devices.reshape(-1, EPG, lanes), ("g", "e", "tp"))
    ep = ("g", "e")
    in_specs = (
        P(ep, None),
        P(ep, None),
        P(ep),
        P(ep, None),
        P(ep),
        P(ep, None),
        P(ep, None, "tp"),
        P(ep, None, "tp"),
        P(ep, "tp", None),
    )
    out_specs = (
        P(ep, "tp"),
        P(ep),
        P(ep, None),
        P(ep, None, "tp"),
        P(ep, None, "tp"),
        P(ep, "tp", None),
    )
    return jax.shard_map(
        shards, mesh=split, in_specs=in_specs, out_specs=out_specs, check_vma=False
    )
```

```python
import functools

import jax
import jax.numpy as jnp
from jax import lax
from jax.experimental import pallas as pl
from jax.experimental.pallas import tpu as pltpu
from jax.sharding import Mesh, PartitionSpec as P

EPG = 4
LANES = 128
VMEM_LIMIT = 36 * 1024 * 1024
FINISH_LIMIT = 16 * 1024 * 1024

MESH = pl.DeviceIdType.MESH

CONTRACT_COLS = (((1,), (1,)), ((), ()))
CONTRACT_ROWS = (((0,), (0,)), ((), ()))


def partner(g, d, groups, sign):
    if groups & (groups - 1):
        return lax.rem(g + sign * d + groups, groups)
    met, bit = g, 1
    while bit < groups:
        if d & bit:
            met = met + bit - 2 * bit * ((g // bit) % 2)
        bit *= 2
    return met


def swapped(g, groups):
    return 0 if groups & (groups - 1) else (g + g // 2) % 2


class Copies:
    def __init__(self, send_sem, recv_sem):
        self.send_sem, self.recv_sem, self.count, self.made = send_sem, recv_sem, 0, []

    def describe(self, src, dst, device, number):
        return pltpu.make_async_remote_copy(
            src_ref=src,
            dst_ref=dst,
            send_sem=self.send_sem.at[number],
            recv_sem=self.recv_sem.at[number],
            device_id=device,
            device_id_type=MESH,
        )

    def reserve(self, count):
        self.count += count
        return self.count - count

    def start(self, src, dst, device):
        copy = self.describe(src, dst, device, self.reserve(1))
        copy.start()
        self.made.append(copy)
        return copy

    def finish(self):
        for copy in self.made:
            copy.wait_send()


def copy_count(groups, lanes):
    far = lanes - 1
    first = (groups - 1) * 3
    spread = (groups - 1) * (2 + 4 * far) + 2 + 2 * far
    inside = groups * 7
    back = groups * (4 + 2 * far) + groups - 1
    return first + spread + inside + back


def dot(a, b):
    return jnp.dot(a, b, preferred_element_type=jnp.float32)


def add(*parts):
    total = parts[0].astype(jnp.float32)
    for part in parts[1:]:
        total = total + part.astype(jnp.float32)
    return total.astype(jnp.bfloat16)


def plan(groups):
    steps = [("own", 0), ("relay_t", 0)]
    if groups > 1:
        steps += [("arrive_t", 1), ("relay_c", 0), ("arrive_c", 1), ("relay_t", 1), ("relay_c", 1)]
    else:
        steps += [("relay_c", 0), ("inside_t", 0), ("inside_c", 0), ("compute", 0)]
    for d in range(1, groups):
        more = d + 1 < groups
        if more:
            steps.append(("arrive_t", d + 1))
        if d == 1:
            steps += [("inside_t", 0), ("inside_c", 0), ("compute", 0)]
        steps.append(("inside_t", d))
        if more:
            steps.append(("arrive_c", d + 1))
        steps.append(("inside_c", d))
        if more:
            steps += [("relay_t", d + 1), ("relay_c", d + 1)]
        steps.append(("compute", d))
        if d > 1:
            steps.append(("sum_cores", d - 1))
    order = list(range(1, groups)) + [0]
    stage = {d: 1 for d in range(1, groups - 1)}
    waiting = [d for d in order if d not in stage]
    while stage or waiting:
        if waiting:
            d = waiting.pop(0)
            steps.append(("sum_cores", d))
            stage[d] = 1
        steps.append(("weights", 0))
        for d in [d for d in order if stage.get(d) == 2][:1]:
            steps.append(("last_sum", d))
            del stage[d]
        for d in [d for d in order if stage.get(d) == 1][:1]:
            steps.append(("middle_sum", d))
            stage[d] = 2
    return steps


def kernel(
    groups, lanes, cap, wide0, wide1,
    choice_in, weight_in, weights_in, local_in, tokens_in, cotangent_in, w_gate, w_up, w_down,
    token_grad, gate_grad, grad_first, grad_second, grad_third,
    choice, weight, weights_t, local_t, tokens, cotangent, pick, out_t, out_c, out_g, tok, cot, gate, first, second, third,
    gg, gu, wt, wt_t, part_a, part_b, rc_a, rc_b, s1_a, s1_b, rx_a, rl_a, rl_b, s2_a, s2_b, rx_b,
    done, ret, send, recv, loc,
):
    g, e, y = lax.axis_index("g"), lax.axis_index("e"), lax.axis_index("tp")
    x, c = e // 2, e % 2
    ex, ec = (g, (1 - x) * 2 + c, y), (g, x * 2 + (1 - c), y)
    token_count, feature_count = tokens.shape
    piece = feature_count // lanes
    rows = EPG * cap
    far = range(1, lanes)
    ahead = [lax.rem(y + r, lanes) for r in far]
    behind = [lax.rem(y + lanes - r, lanes) for r in far]
    others = [(g, e, lane) for lane in ahead]

    loads = [
        pltpu.make_async_copy(src, dst, loc.at[i])
        for i, (src, dst) in enumerate(
            (
                (choice_in, choice), (weight_in, weight), (weights_in, weights_t),
                (local_in, local_t), (tokens_in, tokens), (cotangent_in, cotangent),
                (w_gate, first), (w_up, second), (w_down, third),
            )
        )
    ]
    for load in loads:
        load.start()
    barrier = pltpu.get_barrier_semaphore()
    met = [(lax.rem(g + d, groups), e, y) for d in range(1, groups)] + others + [ex, ec]
    for device in met:
        pl.semaphore_signal(barrier, inc=1, device_id=device, device_id_type=MESH)

    def iota(shape, dim):
        return lax.broadcasted_iota(jnp.int32, shape, dim)

    def spread_rows(rows_of, source):
        return dot(rows_of, source).astype(jnp.bfloat16)

    for load in loads[:4]:
        load.wait()
    chosen = choice[...]
    square = (token_count, token_count)
    earlier = (iota(square, 0) < iota(square, 1)).astype(jnp.float32).astype(jnp.bfloat16)
    high = -(-groups // 16) * 16
    named = iota((high, token_count), 0) == chosen
    member = jnp.where(named, 1.0, 0.0)
    rank = jnp.sum(member * dot(member.astype(jnp.bfloat16), earlier), axis=0, keepdims=True)
    rank = jnp.where(rank < cap, rank, cap).astype(jnp.int32)
    dest = chosen * cap + rank
    one_hot = jnp.where(iota((groups * cap, token_count), 0) == dest, 1.0, 0.0).astype(jnp.bfloat16)
    pick[...] = one_hot.reshape(groups, cap, token_count)
    gates = (weight[...] * weights_t[...]).astype(jnp.bfloat16).astype(jnp.float32)
    gate_rows = jnp.zeros((LANES, token_count), jnp.float32)
    for k in range(local_t.shape[0]):
        hit = iota((LANES, token_count), 0) == local_t[k : k + 1, :]
        gate_rows = gate_rows + jnp.where(hit, gates[k : k + 1, :], 0.0)
    columns = pl.ds(pl.multiple_of(y * piece, LANES), piece)
    blocks = lax.dot_general(
        one_hot, gate_rows.astype(jnp.bfloat16), CONTRACT_COLS, preferred_element_type=jnp.float32
    )
    out_g[...] = blocks.astype(jnp.bfloat16).reshape(groups, cap, LANES)
    loads[4].wait()
    out_t[...] = spread_rows(one_hot, tokens[:, columns]).reshape(groups, cap, piece)
    loads[5].wait()
    out_c[...] = spread_rows(one_hot, cotangent[:, columns]).reshape(groups, cap, piece)
    pl.semaphore_wait(barrier, len(met))

    copies = Copies(send, recv)
    state = [dict() for _ in range(groups)]
    base = copies.reserve(3 * (groups - 1))
    flip = swapped(g, groups)

    def cross(d, target):
        there = (target, e, y)
        number = base + 3 * (d - 1)
        return [
            copies.describe(out_t.at[target], tok.at[y, d, 0], there, number),
            copies.describe(out_g.at[target], gate.at[d, 0], there, number + 1),
            copies.describe(out_c.at[target], cot.at[y, d, 0], there, number + 2),
        ]

    for k in range(1, groups):
        d, target = k, partner(g, k, groups, -1)
        if k > 1 and not isinstance(flip, int):
            d = k + flip * (1 - 2 * (k % 2))
            target = target + flip * (1 - 2 * (target % 2))
        for copy in cross(d, target):
            copy.start()
    for d in range(1, groups):
        arriving = cross(d, partner(g, d, groups, -1))
        copies.made += arriving
        state[d]["zt"], state[d]["zg"], state[d]["zc"] = arriving

    def own(_):
        s = state[0]
        s["tx"] = [copies.start(out_t.at[g], tok.at[y, 0, 1], ex)]
        s["gx"] = copies.start(out_g.at[g], gate.at[0, 1], ex)
        s["cx"] = copies.start(out_c.at[g], cot.at[y, 0, 1], ex)
        mine = pick[g]
        for lane in range(lanes):
            cols = slice(lane * piece, (lane + 1) * piece)
            tok[lane, 0, 0] = spread_rows(mine, tokens[:, cols])
            cot[lane, 0, 0] = spread_rows(mine, cotangent[:, cols])
        gate[0, 0] = out_g[g]
        s["core"] = [
            copies.start(out_g.at[g], gate.at[0, 2], ec),
            copies.start(tok.at[:, 0, 0], tok.at[:, 0, 2], ec),
            copies.start(cot.at[:, 0, 0], cot.at[:, 0, 2], ec),
        ]

    def arrive_t(d):
        s = state[d]
        s["zt"].wait_recv()
        mine = tok.at[y, d, 0]
        s["tl"] = [copies.start(mine, mine, device) for device in others]
        s["tx"] = [copies.start(mine, tok.at[y, d, 1], ex)]
        s["zg"].wait_recv()
        s["gx"] = copies.start(gate.at[d, 0], gate.at[d, 1], ex)
        s["core"] = [copies.start(gate.at[d, 0], gate.at[d, 2], ec)]

    def arrive_c(d):
        s = state[d]
        s["zc"].wait_recv()
        mine = cot.at[y, d, 0]
        s["cx"] = copies.start(mine, cot.at[y, d, 1], ex)
        s["cl"] = [copies.start(mine, mine, device) for device in others]

    def relay_t(d):
        s = state[d]
        if d == 0:
            s["tx"][0].wait_recv()
            theirs = tok.at[y, 0, 1]
            s["txl"] = [copies.start(theirs, theirs, device) for device in others]
        else:
            for i, copy in enumerate(s["tl"]):
                copy.wait_recv()
                theirs = tok.at[behind[i], d, 0]
                s["tx"].append(copies.start(theirs, tok.at[behind[i], d, 1], ex))
            s["core"].append(copies.start(tok.at[:, d, 0], tok.at[:, d, 2], ec))

    def relay_c(d):
        s = state[d]
        s["cx"].wait_recv()
        theirs = cot.at[y, d, 1]
        s["cxl"] = [copies.start(theirs, theirs, device) for device in others]

    def inside_t(d):
        s = state[d]
        if d == 0:
            for copy in s["txl"]:
                copy.wait_recv()
        else:
            for copy in s["cl"]:
                copy.wait_recv()
            s["core"].append(copies.start(cot.at[:, d, 0], cot.at[:, d, 2], ec))
            for copy in s["tx"]:
                copy.wait_recv()
        s["core"].append(copies.start(tok.at[:, d, 1], tok.at[:, d, 3], ec))

    def inside_c(d):
        s = state[d]
        s["gx"].wait_recv()
        s["core"].append(copies.start(gate.at[d, 1], gate.at[d, 3], ec))
        for copy in s["cxl"]:
            copy.wait_recv()
        s["core"].append(copies.start(cot.at[:, d, 1], cot.at[:, d, 3], ec))

    loaded = []

    def compute(d):
        s = state[d]
        if not loaded:
            for load in loads[6:]:
                load.wait()
            loaded.append(True)
        for copy in s["core"]:
            copy.wait_recv()
        pre_gate = pre_up = back = None
        for lane in range(lanes):
            cols = slice(lane * piece, (lane + 1) * piece)
            rows_t = tok[lane, d].reshape(rows, piece)
            rows_c = cot[lane, d].reshape(rows, piece)
            one = dot(rows_t, first[cols, :])
            two = dot(rows_t, second[cols, :])
            three = lax.dot_general(
                rows_c, third[:, cols], CONTRACT_COLS, preferred_element_type=jnp.float32
            )
            pre_gate = one if lane == 0 else pre_gate + one
            pre_up = two if lane == 0 else pre_up + two
            back = three if lane == 0 else back + three
        own_col = iota((rows, LANES), 1) == e
        gates = gate[d].reshape(rows, LANES).astype(jnp.float32)
        gate_float = jnp.sum(jnp.where(own_col, gates, 0.0), axis=1, keepdims=True)
        sigma = jax.nn.sigmoid(pre_gate)
        swish = pre_gate * sigma
        hidden = swish * pre_up
        gate_part = jnp.sum(hidden * back, axis=1, keepdims=True)
        scaled = gate_float * back
        grad_gate = (scaled * pre_up * sigma * (1.0 + pre_gate * (1.0 - sigma))).astype(jnp.bfloat16)
        grad_up = (scaled * swish).astype(jnp.bfloat16)
        at = slice(d * rows, (d + 1) * rows)
        gg[at, :] = grad_gate
        gu[at, :] = grad_up
        wt[at, :] = (gate_float * hidden).astype(jnp.bfloat16)
        gate_out = jnp.where(own_col, gate_part, 0.0).astype(jnp.bfloat16)

        def rows_back(lo, hi):
            total = lax.dot_general(
                grad_gate, first[lo:hi, :], CONTRACT_COLS, preferred_element_type=jnp.float32
            ) + lax.dot_general(
                grad_up, second[lo:hi, :], CONTRACT_COLS, preferred_element_type=jnp.float32
            )
            return total.astype(jnp.bfloat16).reshape(EPG, cap, hi - lo)

        for lane in range(lanes):
            lo = lane * piece
            part_a[d, lane] = rows_back(lo, lo + wide0)
            if wide0 < piece:
                part_b[d, lane, :, :, : piece - wide0] = rows_back(lo + wide0, lo + piece)
            part_b[d, lane, :, :, piece - wide0 :] = gate_out.reshape(EPG, cap, LANES)
        s["pa"] = copies.start(part_a.at[d, :, pl.ds(2, 2)], rc_a.at[d], ec)
        s["pb"] = copies.start(part_b.at[d, :, pl.ds(2, 2)], rc_b.at[d], ec)

    def sum_cores(d):
        s = state[d]
        s["pa"].wait_recv()
        s1_a[d] = add(part_a[d, :, 0:2], rc_a[d])
        s["x0"] = copies.start(s1_a.at[d, :, 1], rx_a.at[d], ex)
        s["pb"].wait_recv()
        s1_b[d] = add(part_b[d, :, 0:2], rc_b[d])
        s["l1"] = [
            copies.start(s1_b.at[d, lane], rl_b.at[d, i], (g, e, lane))
            for i, lane in enumerate(ahead)
        ]

    def middle_sum(d):
        s = state[d]
        s["x0"].wait_recv()
        s2_a[d] = add(s1_a[d, :, 0], rx_a[d])
        s["l0"] = [
            copies.start(s2_a.at[d, lane], rl_a.at[d, i], (g, e, lane))
            for i, lane in enumerate(ahead)
        ]
        for copy in s["l1"]:
            copy.wait_recv()
        s2_b[d] = add(s1_b[d, y], *[rl_b[d, i] for i in range(lanes - 1)])
        s["x1"] = copies.start(s2_b.at[d, 1], rx_b.at[d], ex)

    def last_sum(d):
        s = state[d]
        for copy in s["l0"]:
            copy.wait_recv()
        head = add(s2_a[d, y], *[rl_a[d, i] for i in range(lanes - 1)])
        s["x1"].wait_recv()
        tail = add(s2_b[d, 0], rx_b[d])
        if d == 0:
            ret[g, :, :wide0] = head
            ret[g, :, wide0:] = tail
        else:
            done[d, :, :wide0] = head
            done[d, :, wide0:] = tail
            there = (partner(g, d, groups, 1), e, y)
            s["z"] = copies.start(done.at[d], ret.at[g], there)

    tile = min(2 * LANES, piece)
    per = piece // tile
    tiles = feature_count // tile
    seen = [0]

    def weights_to(end):
        if seen[0] == 0 and end > 0:
            wt_t[...] = wt[...].T
        grads_gate, grads_up = gg[...], gu[...]
        left = wt_t[...]

        def turn(i, carry):
            lane, cols = i // per, pl.ds(pl.multiple_of(lax.rem(i, per) * tile, LANES), tile)
            turned = tok[lane, :, :, :, cols].reshape(groups * rows, tile).T
            at = pl.ds(pl.multiple_of(i * tile, LANES), tile)
            grad_first[at, :] = dot(turned, grads_gate)
            grad_second[at, :] = dot(turned, grads_up)
            grad_third[:, at] = dot(left, cot[lane, :, :, :, cols].reshape(groups * rows, tile))
            return carry

        if end > seen[0]:
            lax.fori_loop(seen[0], end, turn, 0)
        seen[0] = end

    steps = plan(groups)
    shares = sum(name == "weights" for name, _ in steps)
    served = [0]

    def weights(_):
        served[0] += 1
        weights_to(tiles * served[0] // shares)

    phases = {
        "own": own, "arrive_t": arrive_t, "arrive_c": arrive_c, "relay_t": relay_t,
        "relay_c": relay_c, "inside_t": inside_t, "inside_c": inside_c, "compute": compute,
        "sum_cores": sum_cores, "middle_sum": middle_sum, "last_sum": last_sum,
        "weights": weights,
    }
    for name, d in steps:
        with jax.named_scope(f"{name}_{d}"):
            phases[name](d)
    with jax.named_scope("gather"):
        for d in range(1, groups):
            state[d]["z"].wait_recv()
        back = ret[...].reshape(groups * cap, wide0 + wide1)
        token_grad[...] = lax.dot_general(
            one_hot, back[:, :piece], CONTRACT_ROWS, preferred_element_type=jnp.float32
        )
        gate_grad[...] = lax.dot_general(
            back[:, piece:], one_hot, CONTRACT_ROWS, preferred_element_type=jnp.float32
        )
    copies.finish()


def route(choice, weight, weights_t, local_t, tokens, cotangent, w_gate, w_up, w_down, groups, lanes, cap):
    token_count, feature_count = tokens.shape
    hidden_count = w_gate.shape[1]
    piece = feature_count // lanes
    wide1 = (piece + LANES) // (2 * LANES) * LANES
    wide0 = piece + LANES - wide1
    rows = EPG * cap
    far = max(lanes - 1, 1)
    count = copy_count(groups, lanes)
    vmem, hbm = pl.BlockSpec(memory_space=pltpu.VMEM), pl.BlockSpec(memory_space=pltpu.HBM)

    def buffer(*shape):
        return pltpu.VMEM(shape, jnp.bfloat16)

    def grad(*shape):
        return jax.ShapeDtypeStruct(shape, jnp.float32)

    return pl.pallas_call(
        functools.partial(kernel, groups, lanes, cap, wide0, wide1),
        out_shape=(
            grad(token_count, piece),
            grad(LANES, token_count),
            grad(feature_count, hidden_count),
            grad(feature_count, hidden_count),
            grad(hidden_count, feature_count),
        ),
        in_specs=[hbm] * 9,
        out_specs=(vmem,) * 5,
        scratch_shapes=[
            pltpu.VMEM(choice.shape, choice.dtype),
            pltpu.VMEM(weight.shape, weight.dtype),
            pltpu.VMEM(weights_t.shape, weights_t.dtype),
            pltpu.VMEM(local_t.shape, local_t.dtype),
            buffer(token_count, feature_count),
            buffer(token_count, feature_count),
            buffer(groups, cap, token_count),
            buffer(groups, cap, piece),
            buffer(groups, cap, piece),
            buffer(groups, cap, LANES),
            buffer(lanes, groups, EPG, cap, piece),
            buffer(lanes, groups, EPG, cap, piece),
            buffer(groups, EPG, cap, LANES),
            buffer(feature_count, hidden_count),
            buffer(feature_count, hidden_count),
            buffer(hidden_count, feature_count),
            buffer(groups * rows, hidden_count),
            buffer(groups * rows, hidden_count),
            buffer(groups * rows, hidden_count),
            buffer(hidden_count, groups * rows),
            buffer(groups, lanes, EPG, cap, wide0),
            buffer(groups, lanes, EPG, cap, wide1),
            buffer(groups, lanes, 2, cap, wide0),
            buffer(groups, lanes, 2, cap, wide1),
            buffer(groups, lanes, 2, cap, wide0),
            buffer(groups, lanes, 2, cap, wide1),
            buffer(groups, lanes, cap, wide0),
            buffer(groups, far, cap, wide0),
            buffer(groups, far, 2, cap, wide1),
            buffer(groups, lanes, cap, wide0),
            buffer(groups, 2, cap, wide1),
            buffer(groups, cap, wide1),
            buffer(groups, cap, wide0 + wide1),
            buffer(groups, cap, wide0 + wide1),
            pltpu.SemaphoreType.DMA((count,)),
            pltpu.SemaphoreType.DMA((count,)),
            pltpu.SemaphoreType.DMA((9,)),
        ],
        compiler_params=pltpu.CompilerParams(
            collective_id=0, has_side_effects=True, vmem_limit_bytes=VMEM_LIMIT
        ),
        name="routed_backward",
    )(choice, weight, weights_t, local_t, tokens, cotangent, w_gate, w_up, w_down)


def finish_kernel(
    weight, weights_t, local_t, gate_grad, token_grad, first, second, third,
    group_out, expert_out, token_out, first_out, second_out, third_out, sem,
):
    moves = [
        pltpu.make_async_copy(src, dst, sem.at[i])
        for i, (src, dst) in enumerate(
            (
                (first, first_out), (second, second_out), (third, third_out),
                (token_grad, token_out),
            )
        )
    ]
    for move in moves:
        move.start()
    total = None
    for k in range(local_t.shape[0]):
        hit = lax.broadcasted_iota(jnp.int32, gate_grad.shape, 0) == local_t[k : k + 1, :]
        held = jnp.sum(jnp.where(hit, gate_grad[...], 0.0), axis=0, keepdims=True)
        held = held.astype(jnp.bfloat16).astype(jnp.float32)
        expert_out[k : k + 1, :] = weight[...] * held
        term = weights_t[k : k + 1, :] * held
        total = term if total is None else total + term
    group_out[...] = total
    for move in moves:
        move.wait()


def finish(weight, weights_t, local_t, gate_grad, token_grad, first, second, third):
    vmem, hbm = pl.BlockSpec(memory_space=pltpu.VMEM), pl.BlockSpec(memory_space=pltpu.HBM)

    def like(array):
        return jax.ShapeDtypeStruct(array.shape, jnp.float32)

    return pl.pallas_call(
        finish_kernel,
        out_shape=(
            like(weight), like(weights_t), like(token_grad), like(first), like(second), like(third)
        ),
        in_specs=[vmem] * 8,
        out_specs=(vmem,) * 2 + (hbm,) * 4,
        scratch_shapes=[pltpu.SemaphoreType.DMA((4,))],
        compiler_params=pltpu.CompilerParams(vmem_limit_bytes=FINISH_LIMIT),
        name="write_results",
    )(weight, weights_t, local_t, gate_grad, token_grad, first, second, third)


def shards(
    tokens, cotangent, group_weight, expert_weight, group_choice, local_choice, w_gate, w_up, w_down
):
    token_count = tokens.shape[0]
    pick_count = expert_weight.shape[1]
    group_count = lax.axis_size("g")
    lane_count = lax.axis_size("tp")
    expert_count = group_count * EPG
    capacity = pick_count * (3 * token_count // (2 * expert_count))
    group_cap = -(-(EPG * capacity // pick_count) // 16) * 16
    weight = group_weight.reshape(1, token_count)
    weights_t, local_t = expert_weight.T, local_choice.T
    operands = (
        group_choice.reshape(1, token_count), weight, weights_t, local_t,
        tokens, cotangent, w_gate[0], w_up[0], w_down[0],
    )
    operands = [pltpu.with_memory_space_constraint(array, pltpu.HBM) for array in operands]
    token_grad, gate_grad, first_grad, second_grad, third_grad = route(
        *operands, group_count, lane_count, group_cap
    )
    group_grad, expert_grad, token_grad, first_grad, second_grad, third_grad = finish(
        weight, weights_t, local_t, gate_grad, token_grad, first_grad, second_grad, third_grad
    )
    return (
        token_grad,
        group_grad.reshape(token_count),
        expert_grad.T,
        first_grad[None],
        second_grad[None],
        third_grad[None],
    )


def solution(mesh):
    lanes = mesh.shape["tp"]
    split = Mesh(mesh.devices.reshape(-1, EPG, lanes), ("g", "e", "tp"))
    ep = ("g", "e")
    in_specs = (
        P(ep, None),
        P(ep, None),
        P(ep),
        P(ep, None),
        P(ep),
        P(ep, None),
        P(ep, None, "tp"),
        P(ep, None, "tp"),
        P(ep, "tp", None),
    )
    out_specs = (
        P(ep, "tp"),
        P(ep),
        P(ep, None),
        P(ep, None, "tp"),
        P(ep, None, "tp"),
        P(ep, "tp", None),
    )
    return jax.shard_map(
        shards, mesh=split, in_specs=in_specs, out_specs=out_specs, check_vma=False
    )
```

```python
import functools

import jax
import jax.numpy as jnp
from jax import lax
from jax.experimental import pallas as pl
from jax.experimental.pallas import tpu as pltpu
from jax.sharding import Mesh, PartitionSpec as P

EPG = 4
LANES = 128
PACKED = 16
SENDS = 32
VMEM_LIMIT = 36 * 1024 * 1024
FINISH_LIMIT = 16 * 1024 * 1024

MESH = pl.DeviceIdType.MESH

CONTRACT_COLS = (((1,), (1,)), ((), ()))
CONTRACT_ROWS = (((0,), (0,)), ((), ()))


def partner(g, d, groups, sign):
    if groups & (groups - 1):
        return lax.rem(g + sign * d + groups, groups)
    met, bit = g, 1
    while bit < groups:
        if d & bit:
            met = met + bit - 2 * bit * ((g // bit) % 2)
        bit *= 2
    return met


def is_inner(g, groups):
    return 0 if groups & (groups - 1) else (g + g // 2) % 2


class Copies:
    def __init__(self, send_sem, recv_sem):
        self.send_sem, self.recv_sem, self.count, self.made = send_sem, recv_sem, 0, []
        self.kept = []

    def describe(self, src, dst, device, number, slot):
        return pltpu.make_async_remote_copy(
            src_ref=src,
            dst_ref=dst,
            send_sem=self.send_sem.at[slot],
            recv_sem=self.recv_sem.at[number],
            device_id=device,
            device_id_type=MESH,
        )

    def reserve(self, count):
        self.count += count
        return self.count - count

    def start(self, src, dst, device, number=None):
        slot = len(self.made) % SENDS
        if len(self.made) >= SENDS:
            self.made[len(self.made) - SENDS].wait_send()
        number = self.reserve(1) if number is None else number
        copy = self.describe(src, dst, device, number, slot)
        copy.start()
        self.made.append(copy)
        return copy

    def finish(self):
        for copy in self.kept + self.made[-SENDS:]:
            copy.wait_send()


def whole_groups(groups, lanes):
    return range(1, min(groups, 2)) if lanes == 2 else range(0)


def copy_count(groups, lanes):
    far = lanes - 1
    whole = len(whole_groups(groups, lanes))
    first = (groups - 1) * 3 + whole * 2 * far
    spread = (groups - 1 - whole) * (2 + 4 * far) + (1 + whole) * (2 + 2 * far)
    inside = groups * 4
    back = groups * (6 + 3 * far) + 2 * (groups - 1)
    return first + spread + inside + back


def dot(a, b):
    return jnp.dot(a, b, preferred_element_type=jnp.float32)


def add(*parts):
    total = parts[0].astype(jnp.float32)
    for part in parts[1:]:
        total = total + part.astype(jnp.float32)
    return total.astype(jnp.bfloat16)


def plan(groups):
    steps = []

    def put(names, d):
        for name in names.split():
            if (0 <= d < groups or name == "weights") and (name, d) not in steps and (d or not name.startswith("arrive")):
                steps.append((name, d))

    put("own relay_t", 0)
    put("arrive_t", 1)
    put("next_t relay_c", 0)
    put("arrive_c relay_t", 1)
    put("next_c", 0)
    put("relay_c", 1)
    put("inside_t inside_c", 0)
    put("arrive_t", 2)
    put("rest_t compute", 0)
    put("inside_t inside_c", 1)
    put("arrive_c", 2)
    put("rest_c", 0)
    put("relay_t", 2)
    put("inside_z", 1)
    put("relay_c", 2)
    for d in range(3, groups):
        put("arrive_t arrive_c", d)
        put("compute", d - 2)
        put("inside_t inside_c", d - 1)
        put("relay_t relay_c", d)
        put("sum_cores", d - 2)
        put("sum_cores", 0)
        put("compute", d - 1)
        if d < groups - 1:
            put("middle_sum last_sum", d - 2)
    last = groups - 1
    before = last - 1 if last > 2 else 0
    put("compute", 1)
    put("inside_t", last)
    if before:
        put("sum_cores", before)
    put("inside_c", last)
    if before:
        put("middle_sum", before - 1)
        put("middle_sum", 0)
    put("compute", last)
    if before:
        put("last_sum", before - 1)
        put("middle_sum", before)
    if last > 0:
        put("sum_cores", last)
    put("weights", 0)
    if before:
        put("last_sum", 0)
    if before:
        put("last_sum", before)
    put("weights", 1)
    if last > 0:
        put("middle_sum", last)
    put("sum_cores", 0)
    if last == 2:
        put("sum_cores middle_sum last_sum", 1)
    put("weights", 2)
    if last > 0:
        put("last_sum", last)
    put("middle_sum", 0)
    put("weights", 3)
    put("last_sum", 0)
    return steps


def kernel(
    groups, lanes, cap, wide0, wide1,
    choice_in, weight_in, weights_in, local_in, tokens_in, cotangent_in, w_gate, w_up, w_down,
    token_grad, gate_grad, grad_first, grad_second, grad_third,
    choice, weight, weights_t, local_t, tokens, cotangent, pick, out_t, out_c, out_g, all_t, all_c, tok, cot, gate, first, second, third,
    gg, gu, wt, wt_t, part_a, part_b, rc_a, rc_b, s1_a, s1_b, rx_a, rl_a, rl_b, s2_a, s2_b, rx_b,
    done, ret, part_g, rc_g, s1_g, rx_g, s2_g, rl_g, done_g, ret_g, send, recv, loc,
):
    g, e, y = lax.axis_index("g"), lax.axis_index("e"), lax.axis_index("tp")
    x, c = e // 2, e % 2
    ex, ec = (g, (1 - x) * 2 + c, y), (g, x * 2 + (1 - c), y)
    token_count, feature_count = tokens.shape
    piece = feature_count // lanes
    rows = EPG * cap
    far = range(1, lanes)
    ahead = [lax.rem(y + r, lanes) for r in far]
    behind = [lax.rem(y + lanes - r, lanes) for r in far]
    others = [(g, e, lane) for lane in ahead]

    loads = [
        pltpu.make_async_copy(src, dst, loc.at[i])
        for i, (src, dst) in enumerate(
            (
                (choice_in, choice), (weight_in, weight), (weights_in, weights_t),
                (local_in, local_t), (tokens_in, tokens), (cotangent_in, cotangent),
                (w_gate, first), (w_up, second), (w_down, third),
            )
        )
    ]
    for load in loads:
        load.start()
    barrier = pltpu.get_barrier_semaphore()
    met = [(lax.rem(g + d, groups), e, y) for d in range(1, groups)] + others + [ex, ec]
    for device in met:
        pl.semaphore_signal(barrier, inc=1, device_id=device, device_id_type=MESH)

    def iota(shape, dim):
        return lax.broadcasted_iota(jnp.int32, shape, dim)

    def spread_rows(rows_of, source):
        return dot(rows_of, source).astype(jnp.bfloat16)

    for load in loads[:4]:
        load.wait()
    chosen = choice[...]
    square = (token_count, token_count)
    earlier = (iota(square, 0) < iota(square, 1)).astype(jnp.float32).astype(jnp.bfloat16)
    high = -(-groups // 16) * 16
    named = iota((high, token_count), 0) == chosen
    member = jnp.where(named, 1.0, 0.0)
    rank = jnp.sum(member * dot(member.astype(jnp.bfloat16), earlier), axis=0, keepdims=True)
    rank = jnp.where(rank < cap, rank, cap).astype(jnp.int32)
    dest = chosen * cap + rank
    one_hot = jnp.where(iota((groups * cap, token_count), 0) == dest, 1.0, 0.0).astype(jnp.bfloat16)
    pick[...] = one_hot.reshape(groups, cap, token_count)
    gates = (weight[...] * weights_t[...]).astype(jnp.bfloat16).astype(jnp.float32)
    gate_rows = jnp.zeros((LANES, token_count), jnp.float32)
    for k in range(local_t.shape[0]):
        hit = iota((LANES, token_count), 0) == local_t[k : k + 1, :]
        gate_rows = gate_rows + jnp.where(hit, gates[k : k + 1, :], 0.0)
    columns = pl.ds(pl.multiple_of(y * piece, LANES), piece)
    blocks = lax.dot_general(
        one_hot, gate_rows.astype(jnp.bfloat16), CONTRACT_COLS, preferred_element_type=jnp.float32
    )
    out_g[...] = blocks.astype(jnp.bfloat16).reshape(groups, cap, LANES)
    loads[4].wait()
    out_t[...] = spread_rows(one_hot, tokens[:, columns]).reshape(groups, cap, piece)
    loads[5].wait()
    out_c[...] = spread_rows(one_hot, cotangent[:, columns]).reshape(groups, cap, piece)
    whole = whole_groups(groups, lanes)
    pl.semaphore_wait(barrier, len(met))

    copies = Copies(send, recv)
    state = [dict() for _ in range(groups)]
    base = copies.reserve(3 * (groups - 1))

    def cross(d, target):
        there = (target, e, y)
        number = base + 3 * (d - 1)
        return [
            copies.describe(out_t.at[target], tok.at[y, d, 0], there, number, SENDS + number),
            copies.describe(out_g.at[target], gate.at[d, 0], there, number + 1, SENDS + number + 1),
            copies.describe(out_c.at[target], cot.at[y, d, 0], there, number + 2, SENDS + number + 2),
        ]

    def send(ds, kinds):
        for d in ds:
            for kind in kinds:
                cross(d, partner(g, d, groups, -1))[kind].start()

    inner = is_inner(g, groups)
    far_first = groups > 3 and not isinstance(inner, int)
    send(range(1, min(groups, 2)), (0, 1, 2))
    if far_first:
        pl.when(inner == 1)(lambda: send([3], (0, 1, 2)))
    for d in whole:
        mine = pick[partner(g, d, groups, -1)]
        for lane in range(lanes):
            cols = slice(lane * piece, (lane + 1) * piece)
            all_t[d, lane] = spread_rows(mine, tokens[:, cols])
            all_c[d, lane] = spread_rows(mine, cotangent[:, cols])

    def send_whole(source, target, name):
        for d in whole:
            there = (partner(g, d, groups, -1), e, y)
            state[d][name] = [
                copies.start(source.at[d, lane], target.at[lane, d, 0], there) for lane in ahead
            ]

    def next_t(_):
        send(range(2, min(groups, 3)), (0, 1))
        send_whole(all_t, tok, "zat")

    def next_c(_):
        send(range(2, min(groups, 3)), (2,))
        send_whole(all_c, cot, "zac")

    def rest(kinds):
        if far_first:
            pl.when(inner == 0)(lambda: send([3], kinds))
        send(range(4 if far_first else 3, groups), kinds)

    def rest_t(_):
        rest((0, 1))

    def rest_c(_):
        rest((2,))

    for d in range(1, groups):
        arriving = cross(d, partner(g, d, groups, -1))
        copies.kept += arriving
        state[d]["zt"], state[d]["zg"], state[d]["zc"] = arriving

    inner_base = copies.reserve(3 * groups)

    def to_core(d, kind, slot):
        ref = (tok, gate, cot)[kind]
        if kind == 1:
            src, dst = gate.at[d, slot], gate.at[d, slot + 2]
        else:
            src, dst = ref.at[:, d, slot], ref.at[:, d, slot + 2]
        copies.start(src, dst, ec, inner_base + 3 * d + kind)

    def wait_core(d):
        for kind, ref in enumerate((tok, gate, cot)):
            if kind == 1:
                src, dst = gate.at[d, pl.ds(0, 2)], gate.at[d, pl.ds(2, 2)]
            else:
                src, dst = ref.at[:, d, pl.ds(0, 2)], ref.at[:, d, pl.ds(2, 2)]
            copies.describe(src, dst, ec, inner_base + 3 * d + kind, 0).wait_recv()

    def own(_):
        s = state[0]
        s["tx"] = [copies.start(out_t.at[g], tok.at[y, 0, 1], ex)]
        s["gx"] = copies.start(out_g.at[g], gate.at[0, 1], ex)
        s["cx"] = copies.start(out_c.at[g], cot.at[y, 0, 1], ex)
        mine = pick[g]
        for lane in range(lanes):
            cols = slice(lane * piece, (lane + 1) * piece)
            tok[lane, 0, 0] = spread_rows(mine, tokens[:, cols])
            cot[lane, 0, 0] = spread_rows(mine, cotangent[:, cols])
        gate[0, 0] = out_g[g]
        for kind in (1, 0, 2):
            to_core(0, kind, 0)

    def arrive_t(d):
        s = state[d]
        s["zt"].wait_recv()
        mine = tok.at[y, d, 0]
        if d not in whole:
            s["tl"] = [copies.start(mine, mine, device) for device in others]
        s["tx"] = [copies.start(mine, tok.at[y, d, 1], ex)]
        s["zg"].wait_recv()
        s["gx"] = copies.start(gate.at[d, 0], gate.at[d, 1], ex)
        to_core(d, 1, 0)

    def arrive_c(d):
        s = state[d]
        s["zc"].wait_recv()
        mine = cot.at[y, d, 0]
        s["cx"] = copies.start(mine, cot.at[y, d, 1], ex)
        if d not in whole:
            s["cl"] = [copies.start(mine, mine, device) for device in others]

    def relay_t(d):
        s = state[d]
        if d == 0 or d in whole:
            s["tx"][0].wait_recv()
            theirs = tok.at[y, d, 1]
            s["txl"] = [copies.start(theirs, theirs, device) for device in others]
        else:
            for i, copy in enumerate(s["tl"]):
                copy.wait_recv()
                theirs = tok.at[behind[i], d, 0]
                s["tx"].append(copies.start(theirs, tok.at[behind[i], d, 1], ex))
            to_core(d, 0, 0)

    def relay_c(d):
        s = state[d]
        s["cx"].wait_recv()
        theirs = cot.at[y, d, 1]
        s["cxl"] = [copies.start(theirs, theirs, device) for device in others]

    def inside_z(d):
        s = state[d]
        if d in whole:
            for copy in s["zat"]:
                copy.wait_recv()
            to_core(d, 0, 0)
            for copy in s["zac"]:
                copy.wait_recv()
            to_core(d, 2, 0)

    def inside_t(d):
        s = state[d]
        if d == 0 or d in whole:
            for copy in s["txl"]:
                copy.wait_recv()
        else:
            for copy in s["cl"]:
                copy.wait_recv()
            to_core(d, 2, 0)
            for copy in s["tx"]:
                copy.wait_recv()
        to_core(d, 0, 1)

    def inside_c(d):
        s = state[d]
        s["gx"].wait_recv()
        to_core(d, 1, 1)
        for copy in s["cxl"]:
            copy.wait_recv()
        to_core(d, 2, 1)

    loaded = []

    def compute(d):
        s = state[d]
        if not loaded:
            for load in loads[6:]:
                load.wait()
            loaded.append(True)
        wait_core(d)
        pre_gate = pre_up = back = None
        for lane in range(lanes):
            cols = slice(lane * piece, (lane + 1) * piece)
            rows_t = tok[lane, d].reshape(rows, piece)
            rows_c = cot[lane, d].reshape(rows, piece)
            one = dot(rows_t, first[cols, :])
            two = dot(rows_t, second[cols, :])
            three = lax.dot_general(
                rows_c, third[:, cols], CONTRACT_COLS, preferred_element_type=jnp.float32
            )
            pre_gate = one if lane == 0 else pre_gate + one
            pre_up = two if lane == 0 else pre_up + two
            back = three if lane == 0 else back + three
        own_col = iota((rows, LANES), 1) == e
        gates = gate[d].reshape(rows, LANES).astype(jnp.float32)
        gate_float = jnp.sum(jnp.where(own_col, gates, 0.0), axis=1, keepdims=True)
        sigma = jax.nn.sigmoid(pre_gate)
        swish = pre_gate * sigma
        hidden = swish * pre_up
        gate_part = jnp.sum(hidden * back, axis=1, keepdims=True)
        scaled = gate_float * back
        grad_gate = (scaled * pre_up * sigma * (1.0 + pre_gate * (1.0 - sigma))).astype(jnp.bfloat16)
        grad_up = (scaled * swish).astype(jnp.bfloat16)
        at = slice(d * rows, (d + 1) * rows)
        gg[at, :] = grad_gate
        gu[at, :] = grad_up
        wt[at, :] = (gate_float * hidden).astype(jnp.bfloat16)
        gate_out = jnp.where(own_col, gate_part, 0.0).astype(jnp.bfloat16)

        packed_width = part_g.shape[3]
        blocks = gate_out.reshape(EPG, cap, LANES)
        if packed_width > cap:
            filler = jnp.zeros((EPG, packed_width - cap, LANES), jnp.bfloat16)
            blocks = jnp.concatenate([blocks, filler], axis=1)
        chooser = jnp.where(iota((PACKED, LANES), 0) == iota((PACKED, LANES), 1), 1.0, 0.0)
        packed = lax.dot_general(
            chooser.astype(jnp.bfloat16),
            blocks.reshape(EPG * packed_width, LANES),
            CONTRACT_COLS,
            preferred_element_type=jnp.float32,
        ).astype(jnp.bfloat16)
        for slot in range(EPG):
            part_g[d, slot] = packed[:, slot * packed_width : (slot + 1) * packed_width]
        s["pg"] = copies.start(part_g.at[d, pl.ds(2, 2)], rc_g.at[d], ec)
        shares = 2 if d == groups - 1 else 1
        kept = EPG // shares

        def rows_back(lo, hi, half):
            part = slice(half * rows // shares, (half + 1) * rows // shares)
            total = lax.dot_general(
                grad_gate[part], first[lo:hi, :], CONTRACT_COLS, preferred_element_type=jnp.float32
            ) + lax.dot_general(
                grad_up[part], second[lo:hi, :], CONTRACT_COLS, preferred_element_type=jnp.float32
            )
            return total.astype(jnp.bfloat16).reshape(kept, cap, hi - lo)

        for half in reversed(range(shares)):
            slots = slice(half * kept, (half + 1) * kept)
            for lane in range(lanes):
                lo = lane * piece
                part_a[d, lane, slots] = rows_back(lo, lo + wide0, half)
            if half == shares - 1:
                s["pa"] = copies.start(part_a.at[d, :, pl.ds(2, 2)], rc_a.at[d], ec)
            for lane in range(lanes):
                lo = lane * piece
                if wide1:
                    part_b[d, lane, slots] = rows_back(lo + wide0, lo + piece, half)
            if half == shares - 1 and wide1:
                s["pb"] = copies.start(part_b.at[d, :, pl.ds(2, 2)], rc_b.at[d], ec)

    def sum_cores(d):
        s = state[d]
        s["pa"].wait_recv()
        s1_a[d] = add(part_a[d, :, 0:2], rc_a[d])
        s["x0"] = copies.start(s1_a.at[d, :, 1], rx_a.at[d], ex)
        s["pg"].wait_recv()
        s1_g[d] = add(part_g[d, 0:2], rc_g[d])
        s["xg"] = copies.start(s1_g.at[d, 1], rx_g.at[d], ex)
        if wide1:
            s["pb"].wait_recv()
            s1_b[d] = add(part_b[d, :, 0:2], rc_b[d])
            s["l1"] = [
                copies.start(s1_b.at[d, lane], rl_b.at[d, i], (g, e, lane))
                for i, lane in enumerate(ahead)
            ]

    def middle_sum(d):
        s = state[d]
        s["x0"].wait_recv()
        s2_a[d] = add(s1_a[d, :, 0], rx_a[d])
        s["l0"] = [
            copies.start(s2_a.at[d, lane], rl_a.at[d, i], (g, e, lane))
            for i, lane in enumerate(ahead)
        ]
        s["xg"].wait_recv()
        s2_g[d] = add(s1_g[d, 0], rx_g[d])
        s["lg"] = [
            copies.start(s2_g.at[d], rl_g.at[d, i], (g, e, lane)) for i, lane in enumerate(ahead)
        ]
        if wide1:
            for copy in s["l1"]:
                copy.wait_recv()
            s2_b[d] = add(s1_b[d, y], *[rl_b[d, i] for i in range(lanes - 1)])
            s["x1"] = copies.start(s2_b.at[d, 1], rx_b.at[d], ex)

    def last_sum(d):
        s = state[d]
        rows_at, gates_at, at = (ret, ret_g, g) if d == 0 else (done, done_g, d)
        for copy in s["l0"]:
            copy.wait_recv()
        rows_at[at, :, :wide0] = add(s2_a[d, y], *[rl_a[d, i] for i in range(lanes - 1)])
        for copy in s["lg"]:
            copy.wait_recv()
        gates_at[at] = add(s2_g[d], *[rl_g[d, i] for i in range(lanes - 1)])
        if wide1:
            s["x1"].wait_recv()
            rows_at[at, :, wide0:] = add(s2_b[d, 0], rx_b[d])
        if d:
            there = (partner(g, d, groups, 1), e, y)
            s["z"] = [
                copies.start(done.at[d], ret.at[g], there),
                copies.start(done_g.at[d], ret_g.at[g], there),
            ]

    tile = min(2 * LANES, piece)
    per = piece // tile
    tiles = feature_count // tile
    seen = [0]

    def weights_to(end):
        if seen[0] == 0 and end > 0:
            wt_t[...] = wt[...].T
        grads_gate, grads_up = gg[...], gu[...]
        left = wt_t[...]

        def turn(i, carry):
            lane, cols = i // per, pl.ds(pl.multiple_of(lax.rem(i, per) * tile, LANES), tile)
            turned = tok[lane, :, :, :, cols].reshape(groups * rows, tile).T
            at = pl.ds(pl.multiple_of(i * tile, LANES), tile)
            grad_first[at, :] = dot(turned, grads_gate)
            grad_second[at, :] = dot(turned, grads_up)
            grad_third[:, at] = dot(left, cot[lane, :, :, :, cols].reshape(groups * rows, tile))
            return carry

        if end > seen[0]:
            lax.fori_loop(seen[0], end, turn, 0)
        seen[0] = end

    steps = plan(groups)
    shares = sum(name == "weights" for name, _ in steps)
    served = [0]

    def weights(_):
        served[0] += 1
        weights_to(tiles * served[0] // shares)

    phases = {
        "own": own, "arrive_t": arrive_t, "arrive_c": arrive_c, "relay_t": relay_t,
        "relay_c": relay_c, "inside_t": inside_t, "inside_z": inside_z, "inside_c": inside_c, "compute": compute,
        "sum_cores": sum_cores, "middle_sum": middle_sum, "last_sum": last_sum,
        "weights": weights, "next_t": next_t, "next_c": next_c, "rest_t": rest_t, "rest_c": rest_c,
    }
    for name, d in steps:
        with jax.named_scope(f"{name}_{d}"):
            phases[name](d)
    with jax.named_scope("gather"):
        for d in range(1, groups):
            for copy in state[d]["z"]:
                copy.wait_recv()
        token_grad[...] = lax.dot_general(
            one_hot, ret[...].reshape(groups * cap, piece), CONTRACT_ROWS,
            preferred_element_type=jnp.float32,
        )
        total = dot(ret_g[0, :, :cap], pick[0])
        for group in range(1, groups):
            total = total + dot(ret_g[group, :, :cap], pick[group])
        gate_grad[...] = total
    with jax.named_scope("finish"):
        copies.finish()


def route(choice, weight, weights_t, local_t, tokens, cotangent, w_gate, w_up, w_down, groups, lanes, cap):
    token_count, feature_count = tokens.shape
    hidden_count = w_gate.shape[1]
    piece = feature_count // lanes
    wide1 = piece // (2 * LANES) * LANES
    wide0 = piece - wide1
    tail = max(wide1, LANES)
    packed = -(-cap // LANES) * LANES
    rows = EPG * cap
    far = max(lanes - 1, 1)
    count = copy_count(groups, lanes)
    vmem, hbm = pl.BlockSpec(memory_space=pltpu.VMEM), pl.BlockSpec(memory_space=pltpu.HBM)

    def buffer(*shape):
        return pltpu.VMEM(shape, jnp.bfloat16)

    def grad(*shape):
        return jax.ShapeDtypeStruct(shape, jnp.float32)

    return pl.pallas_call(
        functools.partial(kernel, groups, lanes, cap, wide0, wide1),
        out_shape=(
            grad(token_count, piece),
            grad(PACKED, token_count),
            grad(feature_count, hidden_count),
            grad(feature_count, hidden_count),
            grad(hidden_count, feature_count),
        ),
        in_specs=[hbm] * 9,
        out_specs=(vmem,) * 5,
        scratch_shapes=[
            pltpu.VMEM(choice.shape, choice.dtype),
            pltpu.VMEM(weight.shape, weight.dtype),
            pltpu.VMEM(weights_t.shape, weights_t.dtype),
            pltpu.VMEM(local_t.shape, local_t.dtype),
            buffer(token_count, feature_count),
            buffer(token_count, feature_count),
            buffer(groups, cap, token_count),
            buffer(groups, cap, piece),
            buffer(groups, cap, piece),
            buffer(groups, cap, LANES),
            buffer(2, lanes, cap, piece),
            buffer(2, lanes, cap, piece),
            buffer(lanes, groups, EPG, cap, piece),
            buffer(lanes, groups, EPG, cap, piece),
            buffer(groups, EPG, cap, LANES),
            buffer(feature_count, hidden_count),
            buffer(feature_count, hidden_count),
            buffer(hidden_count, feature_count),
            buffer(groups * rows, hidden_count),
            buffer(groups * rows, hidden_count),
            buffer(groups * rows, hidden_count),
            buffer(hidden_count, groups * rows),
            buffer(groups, lanes, EPG, cap, wide0),
            buffer(groups, lanes, EPG, cap, tail),
            buffer(groups, lanes, 2, cap, wide0),
            buffer(groups, lanes, 2, cap, tail),
            buffer(groups, lanes, 2, cap, wide0),
            buffer(groups, lanes, 2, cap, tail),
            buffer(groups, lanes, cap, wide0),
            buffer(groups, far, cap, wide0),
            buffer(groups, far, 2, cap, tail),
            buffer(groups, lanes, cap, wide0),
            buffer(groups, 2, cap, tail),
            buffer(groups, cap, tail),
            buffer(groups, cap, piece),
            buffer(groups, cap, piece),
            buffer(groups, EPG, PACKED, packed),
            buffer(groups, 2, PACKED, packed),
            buffer(groups, 2, PACKED, packed),
            buffer(groups, PACKED, packed),
            buffer(groups, PACKED, packed),
            buffer(groups, far, PACKED, packed),
            buffer(groups, PACKED, packed),
            buffer(groups, PACKED, packed),
            pltpu.SemaphoreType.DMA((SENDS + 3 * max(groups - 1, 1),)),
            pltpu.SemaphoreType.DMA((count,)),
            pltpu.SemaphoreType.DMA((9,)),
        ],
        compiler_params=pltpu.CompilerParams(
            collective_id=0, has_side_effects=True, vmem_limit_bytes=VMEM_LIMIT
        ),
        name="routed_backward",
    )(choice, weight, weights_t, local_t, tokens, cotangent, w_gate, w_up, w_down)


def finish_kernel(
    weight, weights_t, local_t, gate_grad, token_grad, first, second, third,
    group_out, expert_out, token_out, first_out, second_out, third_out, sem,
):
    moves = [
        pltpu.make_async_copy(src, dst, sem.at[i])
        for i, (src, dst) in enumerate(
            (
                (first, first_out), (second, second_out), (third, third_out),
                (token_grad, token_out),
            )
        )
    ]
    for move in moves:
        move.start()
    total = None
    for k in range(local_t.shape[0]):
        hit = lax.broadcasted_iota(jnp.int32, gate_grad.shape, 0) == local_t[k : k + 1, :]
        held = jnp.sum(jnp.where(hit, gate_grad[...], 0.0), axis=0, keepdims=True)
        held = held.astype(jnp.bfloat16).astype(jnp.float32)
        expert_out[k : k + 1, :] = weight[...] * held
        term = weights_t[k : k + 1, :] * held
        total = term if total is None else total + term
    group_out[...] = total
    for move in moves:
        move.wait()


def finish(weight, weights_t, local_t, gate_grad, token_grad, first, second, third):
    vmem, hbm = pl.BlockSpec(memory_space=pltpu.VMEM), pl.BlockSpec(memory_space=pltpu.HBM)

    def like(array):
        return jax.ShapeDtypeStruct(array.shape, jnp.float32)

    return pl.pallas_call(
        finish_kernel,
        out_shape=(
            like(weight), like(weights_t), like(token_grad), like(first), like(second), like(third)
        ),
        in_specs=[vmem] * 8,
        out_specs=(vmem,) * 2 + (hbm,) * 4,
        scratch_shapes=[pltpu.SemaphoreType.DMA((4,))],
        compiler_params=pltpu.CompilerParams(vmem_limit_bytes=FINISH_LIMIT),
        name="write_results",
    )(weight, weights_t, local_t, gate_grad, token_grad, first, second, third)


def shards(
    tokens, cotangent, group_weight, expert_weight, group_choice, local_choice, w_gate, w_up, w_down
):
    token_count = tokens.shape[0]
    pick_count = expert_weight.shape[1]
    group_count = lax.axis_size("g")
    lane_count = lax.axis_size("tp")
    expert_count = group_count * EPG
    capacity = pick_count * (3 * token_count // (2 * expert_count))
    group_cap = -(-(EPG * capacity // pick_count) // 16) * 16
    weight = group_weight.reshape(1, token_count)
    weights_t, local_t = expert_weight.T, local_choice.T
    operands = (
        group_choice.reshape(1, token_count), weight, weights_t, local_t,
        tokens, cotangent, w_gate[0], w_up[0], w_down[0],
    )
    operands = [pltpu.with_memory_space_constraint(array, pltpu.HBM) for array in operands]
    token_grad, gate_grad, first_grad, second_grad, third_grad = route(
        *operands, group_count, lane_count, group_cap
    )
    group_grad, expert_grad, token_grad, first_grad, second_grad, third_grad = finish(
        weight, weights_t, local_t, gate_grad, token_grad, first_grad, second_grad, third_grad
    )
    return (
        token_grad,
        group_grad.reshape(token_count),
        expert_grad.T,
        first_grad[None],
        second_grad[None],
        third_grad[None],
    )


def solution(mesh):
    lanes = mesh.shape["tp"]
    split = Mesh(mesh.devices.reshape(-1, EPG, lanes), ("g", "e", "tp"))
    ep = ("g", "e")
    in_specs = (
        P(ep, None),
        P(ep, None),
        P(ep),
        P(ep, None),
        P(ep),
        P(ep, None),
        P(ep, None, "tp"),
        P(ep, None, "tp"),
        P(ep, "tp", None),
    )
    out_specs = (
        P(ep, "tp"),
        P(ep),
        P(ep, None),
        P(ep, None, "tp"),
        P(ep, None, "tp"),
        P(ep, "tp", None),
    )
    return jax.shard_map(
        shards, mesh=split, in_specs=in_specs, out_specs=out_specs, check_vma=False
    )
```

```python
import functools

import jax
import jax.numpy as jnp
from jax import lax
from jax.experimental import pallas as pl
from jax.experimental.pallas import tpu as pltpu
from jax.sharding import Mesh, PartitionSpec as P

EPG = 4
LANES = 128
PACKED = 16
SENDS = 32
PARTS = 4
VMEM_LIMIT = 36 * 1024 * 1024
FINISH_LIMIT = 16 * 1024 * 1024

MESH = pl.DeviceIdType.MESH

CONTRACT_COLS = (((1,), (1,)), ((), ()))
CONTRACT_ROWS = (((0,), (0,)), ((), ()))


def partner(g, d, groups, sign):
    if groups & (groups - 1):
        return lax.rem(g + sign * d + groups, groups)
    met, bit = g, 1
    while bit < groups:
        if d & bit:
            met = met + bit - 2 * bit * ((g // bit) % 2)
        bit *= 2
    return met


def is_inner(g, groups):
    return 0 if groups & (groups - 1) else (g + g // 2) % 2


class Copies:
    def __init__(self, send_sem, recv_sem):
        self.send_sem, self.recv_sem, self.count, self.made = send_sem, recv_sem, 0, []
        self.kept = []

    def describe(self, src, dst, device, number, slot):
        return pltpu.make_async_remote_copy(
            src_ref=src,
            dst_ref=dst,
            send_sem=self.send_sem.at[slot],
            recv_sem=self.recv_sem.at[number],
            device_id=device,
            device_id_type=MESH,
        )

    def reserve(self, count):
        self.count += count
        return self.count - count

    def start(self, src, dst, device, number=None):
        slot = len(self.made) % SENDS
        if len(self.made) >= SENDS:
            self.made[len(self.made) - SENDS].wait_send()
        number = self.reserve(1) if number is None else number
        copy = self.describe(src, dst, device, number, slot)
        copy.start()
        self.made.append(copy)
        return copy

    def finish(self):
        for copy in self.kept + self.made[-SENDS:]:
            copy.wait_send()


def whole_groups(groups, lanes):
    return range(1, min(groups, 2)) if lanes == 2 else range(0)


def copy_count(groups, lanes):
    far = lanes - 1
    whole = len(whole_groups(groups, lanes))
    first = (groups - 1) * 3 + whole * 2 * far
    spread = (groups - 1 - whole) * (2 + 4 * far) + (1 + whole) * (2 + 2 * far)
    inside = groups * 4
    back = groups * (6 + 3 * far) + 3 * (groups - 1)
    return first + spread + inside + back


def dot(a, b):
    return jnp.dot(a, b, preferred_element_type=jnp.float32)


def add(*parts):
    total = parts[0].astype(jnp.float32)
    for part in parts[1:]:
        total = total + part.astype(jnp.float32)
    return total.astype(jnp.bfloat16)


def plan(groups):
    steps = []

    def put(names, d):
        for name in names.split():
            if (0 <= d < groups or name == "weights") and (name, d) not in steps and (d or not name.startswith("arrive")):
                steps.append((name, d))

    put("own next_t relay_t", 0)
    put("arrive_t", 1)
    put("relay_c", 0)
    put("arrive_c relay_t", 1)
    put("next_c", 0)
    put("relay_c", 1)
    put("inside_t inside_c", 0)
    put("arrive_t", 2)
    put("rest_t compute", 0)
    put("inside_t inside_c", 1)
    put("arrive_c", 2)
    put("rest_c", 0)
    put("relay_t", 2)
    put("inside_z", 1)
    put("arrive_t", 3)
    put("relay_c", 2)
    for d in range(3, groups):
        put("arrive_t arrive_c", d)
        put("compute", d - 2)
        put("inside_t inside_c", d - 1)
        put("relay_t relay_c", d)
        put("sum_cores", d - 2)
        put("sum_cores", 0)
        put("compute", d - 1)
        if d < groups - 1:
            put("middle_sum last_sum", d - 2)
    last = groups - 1
    before = last - 1 if last > 2 else 0
    put("compute", 1)
    put("inside_t", last)
    if before:
        put("sum_cores", before)
    put("inside_c", last)
    if last > 1:
        put("compute_t", last)
    if before:
        put("middle_sum", before - 1)
    put("compute", last)
    if before:
        put("middle_sum", before)
    if last > 0:
        put("sum_cores", last)
    put("weights", 0)
    if before:
        put("last_sum", before - 1)
        put("middle_sum", 0)
    if before:
        put("last_sum", before)
    put("weights", 1)
    if last > 0:
        put("middle_sum", last)
    put("sum_cores", 0)
    if last == 2:
        put("sum_cores middle_sum last_sum", 1)
    put("weights", 2)
    if last > 0:
        put("last_sum", last)
    put("middle_sum last_sum", 0)
    put("weights", 3)
    return steps


def kernel(
    groups, lanes, cap, wide0, wide1,
    choice_in, weight_in, weights_in, local_in, tokens_in, cotangent_in, w_gate, w_up, w_down,
    token_grad, gate_grad, grad_first, grad_second, grad_third,
    choice, weight, weights_t, local_t, tokens, cotangent, pick, out_t, out_c, out_g, all_t, all_c, tok, cot, gate, first, second, third,
    pre, gg, gu, wt, wt_t, part_a, part_b, rc_a, rc_b, s1_a, s1_b, rx_a, rl_a, rl_b, s2_a, s2_b, rx_b,
    done, ret, part_g, rc_g, s1_g, rx_g, s2_g, rl_g, done_g, ret_g, send, recv, loc,
):
    g, e, y = lax.axis_index("g"), lax.axis_index("e"), lax.axis_index("tp")
    x, c = e // 2, e % 2
    ex, ec = (g, (1 - x) * 2 + c, y), (g, x * 2 + (1 - c), y)
    token_count, feature_count = tokens.shape
    piece = feature_count // lanes
    rows = EPG * cap
    far = range(1, lanes)
    ahead = [lax.rem(y + r, lanes) for r in far]
    behind = [lax.rem(y + lanes - r, lanes) for r in far]
    others = [(g, e, lane) for lane in ahead]

    loads = [
        pltpu.make_async_copy(src, dst, loc.at[i])
        for i, (src, dst) in enumerate(
            (
                (choice_in, choice), (weight_in, weight), (weights_in, weights_t),
                (local_in, local_t), (tokens_in, tokens), (cotangent_in, cotangent),
                (w_gate, first), (w_up, second), (w_down, third),
            )
        )
    ]
    for load in loads[:6]:
        load.start()
    barrier = pltpu.get_barrier_semaphore()
    met = [(lax.rem(g + d, groups), e, y) for d in range(1, groups)] + others + [ex, ec]
    for device in met:
        pl.semaphore_signal(barrier, inc=1, device_id=device, device_id_type=MESH)

    def iota(shape, dim):
        return lax.broadcasted_iota(jnp.int32, shape, dim)

    def spread_rows(rows_of, source):
        return dot(rows_of, source).astype(jnp.bfloat16)

    for load in loads[:4]:
        load.wait()
    chosen = choice[...]
    square = (token_count, token_count)
    earlier = (iota(square, 0) < iota(square, 1)).astype(jnp.float32).astype(jnp.bfloat16)
    high = -(-groups // 16) * 16
    named = iota((high, token_count), 0) == chosen
    member = jnp.where(named, 1.0, 0.0)
    rank = jnp.sum(member * dot(member.astype(jnp.bfloat16), earlier), axis=0, keepdims=True)
    rank = jnp.where(rank < cap, rank, cap).astype(jnp.int32)
    dest = chosen * cap + rank
    one_hot = jnp.where(iota((groups * cap, token_count), 0) == dest, 1.0, 0.0).astype(jnp.bfloat16)
    pick[...] = one_hot.reshape(groups, cap, token_count)
    gates = (weight[...] * weights_t[...]).astype(jnp.bfloat16).astype(jnp.float32)
    gate_rows = jnp.zeros((PACKED, token_count), jnp.float32)
    for k in range(local_t.shape[0]):
        hit = iota((PACKED, token_count), 0) == local_t[k : k + 1, :]
        gate_rows = gate_rows + jnp.where(hit, gates[k : k + 1, :], 0.0)
    columns = pl.ds(pl.multiple_of(y * piece, LANES), piece)
    packed_width = out_g.shape[2]
    wide_dest = chosen * packed_width + rank
    wide_hot = iota((groups * packed_width, token_count), 0) == wide_dest
    blocks = lax.dot_general(
        gate_rows.astype(jnp.bfloat16),
        jnp.where(wide_hot, 1.0, 0.0).astype(jnp.bfloat16),
        CONTRACT_COLS,
        preferred_element_type=jnp.float32,
    ).astype(jnp.bfloat16)
    for group in range(groups):
        out_g[group] = blocks[:, group * packed_width : (group + 1) * packed_width]
    loads[4].wait()
    out_t[...] = spread_rows(one_hot, tokens[:, columns]).reshape(groups, cap, piece)
    loads[5].wait()
    out_c[...] = spread_rows(one_hot, cotangent[:, columns]).reshape(groups, cap, piece)
    whole = whole_groups(groups, lanes)
    pl.semaphore_wait(barrier, len(met))

    copies = Copies(send, recv)
    state = [dict() for _ in range(groups)]
    base = copies.reserve(3 * (groups - 1))

    def cross(d, target):
        there = (target, e, y)
        number = base + 3 * (d - 1)
        return [
            copies.describe(out_t.at[target], tok.at[y, d, 0], there, number, SENDS + number),
            copies.describe(out_g.at[target], gate.at[d, 0], there, number + 1, SENDS + number + 1),
            copies.describe(out_c.at[target], cot.at[y, d, 0], there, number + 2, SENDS + number + 2),
        ]

    def send(ds, kinds):
        for d in ds:
            for kind in kinds:
                cross(d, partner(g, d, groups, -1))[kind].start()

    inner = is_inner(g, groups)
    far_first = groups > 3 and not isinstance(inner, int)
    send(range(1, min(groups, 2)), (0, 1, 2))
    if far_first:
        pl.when(inner == 1)(lambda: send([3], (0, 1, 2)))
    for load in loads[6:]:
        load.start()

    def fill_whole():
        for d in whole:
            mine = pick[partner(g, d, groups, -1)]
            for lane in ahead:
                cols = pl.ds(pl.multiple_of(lane * piece, LANES), piece)
                all_t[d, lane] = spread_rows(mine, tokens[:, cols])
                all_c[d, lane] = spread_rows(mine, cotangent[:, cols])

    def send_whole(source, target, name):
        for d in whole:
            there = (partner(g, d, groups, -1), e, y)
            state[d][name] = [
                copies.start(source.at[d, lane], target.at[lane, d, 0], there) for lane in ahead
            ]

    def next_t(_):
        send(range(2, min(groups, 3)), (0, 1))
        send_whole(all_t, tok, "zat")

    def next_c(_):
        send(range(2, min(groups, 3)), (2,))
        send_whole(all_c, cot, "zac")

    def rest(kinds):
        if far_first:
            pl.when(inner == 0)(lambda: send([3], kinds))
        send(range(4 if far_first else 3, groups), kinds)

    def rest_t(_):
        rest((0, 1))

    def rest_c(_):
        rest((2,))

    for d in range(1, groups):
        arriving = cross(d, partner(g, d, groups, -1))
        copies.kept += arriving
        state[d]["zt"], state[d]["zg"], state[d]["zc"] = arriving

    inner_base = copies.reserve(3 * groups)

    def to_core(d, kind, slot):
        ref = (tok, gate, cot)[kind]
        if kind == 1:
            src, dst = gate.at[d, slot], gate.at[d, slot + 2]
        else:
            src, dst = ref.at[:, d, slot], ref.at[:, d, slot + 2]
        copies.start(src, dst, ec, inner_base + 3 * d + kind)

    def wait_core(d, kinds):
        for kind in kinds:
            ref = (tok, gate, cot)[kind]
            if kind == 1:
                src, dst = gate.at[d, pl.ds(0, 2)], gate.at[d, pl.ds(2, 2)]
            else:
                src, dst = ref.at[:, d, pl.ds(0, 2)], ref.at[:, d, pl.ds(2, 2)]
            copies.describe(src, dst, ec, inner_base + 3 * d + kind, 0).wait_recv()

    def own(_):
        s = state[0]
        s["tx"] = [copies.start(out_t.at[g], tok.at[y, 0, 1], ex)]
        s["gx"] = copies.start(out_g.at[g], gate.at[0, 1], ex)
        s["cx"] = copies.start(out_c.at[g], cot.at[y, 0, 1], ex)
        mine = pick[g]
        for lane in range(lanes):
            cols = slice(lane * piece, (lane + 1) * piece)
            tok[lane, 0, 0] = spread_rows(mine, tokens[:, cols])
            cot[lane, 0, 0] = spread_rows(mine, cotangent[:, cols])
        gate[0, 0] = out_g[g]
        for kind in (1, 0, 2):
            to_core(0, kind, 0)
        fill_whole()

    def arrive_t(d):
        s = state[d]
        s["zt"].wait_recv()
        mine = tok.at[y, d, 0]
        if d not in whole:
            s["tl"] = [copies.start(mine, mine, device) for device in others]
        s["tx"] = [copies.start(mine, tok.at[y, d, 1], ex)]
        s["zg"].wait_recv()
        s["gx"] = copies.start(gate.at[d, 0], gate.at[d, 1], ex)
        to_core(d, 1, 0)

    def arrive_c(d):
        s = state[d]
        s["zc"].wait_recv()
        mine = cot.at[y, d, 0]
        s["cx"] = copies.start(mine, cot.at[y, d, 1], ex)
        if d not in whole:
            s["cl"] = [copies.start(mine, mine, device) for device in others]

    def relay_t(d):
        s = state[d]
        if d == 0 or d in whole:
            s["tx"][0].wait_recv()
            theirs = tok.at[y, d, 1]
            s["txl"] = [copies.start(theirs, theirs, device) for device in others]
        else:
            for i, copy in enumerate(s["tl"]):
                copy.wait_recv()
                theirs = tok.at[behind[i], d, 0]
                s["tx"].append(copies.start(theirs, tok.at[behind[i], d, 1], ex))
            to_core(d, 0, 0)

    def relay_c(d):
        s = state[d]
        s["cx"].wait_recv()
        theirs = cot.at[y, d, 1]
        s["cxl"] = [copies.start(theirs, theirs, device) for device in others]

    def inside_z(d):
        s = state[d]
        if d in whole:
            for copy in s["zat"]:
                copy.wait_recv()
            to_core(d, 0, 0)
            for copy in s["zac"]:
                copy.wait_recv()
            to_core(d, 2, 0)

    def inside_t(d):
        s = state[d]
        if d == 0 or d in whole:
            for copy in s["txl"]:
                copy.wait_recv()
        else:
            for copy in s["cl"]:
                copy.wait_recv()
            to_core(d, 2, 0)
            for copy in s["tx"]:
                copy.wait_recv()
        to_core(d, 0, 1)

    def inside_c(d):
        s = state[d]
        s["gx"].wait_recv()
        to_core(d, 1, 1)
        for copy in s["cxl"]:
            copy.wait_recv()
        to_core(d, 2, 1)

    loaded = []

    begun = set()

    def compute_t(d):
        begun.add(d)
        if not loaded:
            for load in loads[6:]:
                load.wait()
            loaded.append(True)
        wait_core(d, (0,))
        for half, weights_in in enumerate((first, second)):
            total = None
            for lane in range(lanes):
                cols = slice(lane * piece, (lane + 1) * piece)
                term = dot(tok[lane, d].reshape(rows, piece), weights_in[cols, :])
                total = term if total is None else total + term
            pre[half] = total

    def compute(d):
        s = state[d]
        if d not in begun:
            compute_t(d)
        wait_core(d, (1, 2))
        back = None
        for lane in range(lanes):
            cols = slice(lane * piece, (lane + 1) * piece)
            term = lax.dot_general(
                cot[lane, d].reshape(rows, piece), third[:, cols], CONTRACT_COLS,
                preferred_element_type=jnp.float32,
            )
            back = term if back is None else back + term
        pre_gate, pre_up = pre[0], pre[1]
        own_col = iota((rows, LANES), 1) == e
        own_row = jnp.where(iota((PACKED, LANES), 0) == e, 1.0, 0.0).astype(jnp.bfloat16)
        gate_float = jnp.concatenate(
            [
                lax.dot_general(
                    gate[d, slot, :, :cap], own_row, CONTRACT_ROWS, preferred_element_type=jnp.float32
                )
                for slot in range(EPG)
            ],
            axis=0,
        )[:, :1]
        sigma = jax.nn.sigmoid(pre_gate)
        swish = pre_gate * sigma
        hidden = swish * pre_up
        gate_part = jnp.sum(hidden * back, axis=1, keepdims=True)
        scaled = gate_float * back
        grad_gate = (scaled * pre_up * sigma * (1.0 + pre_gate * (1.0 - sigma))).astype(jnp.bfloat16)
        grad_up = (scaled * swish).astype(jnp.bfloat16)
        at = slice(d * rows, (d + 1) * rows)
        gg[at, :] = grad_gate
        gu[at, :] = grad_up
        wt[at, :] = (gate_float * hidden).astype(jnp.bfloat16)
        gate_out = jnp.where(own_col, gate_part, 0.0).astype(jnp.bfloat16)

        blocks = gate_out.reshape(EPG, cap, LANES)
        if packed_width > cap:
            filler = jnp.zeros((EPG, packed_width - cap, LANES), jnp.bfloat16)
            blocks = jnp.concatenate([blocks, filler], axis=1)
        chooser = jnp.where(iota((PACKED, LANES), 0) == iota((PACKED, LANES), 1), 1.0, 0.0)
        packed = lax.dot_general(
            chooser.astype(jnp.bfloat16),
            blocks.reshape(EPG * packed_width, LANES),
            CONTRACT_COLS,
            preferred_element_type=jnp.float32,
        ).astype(jnp.bfloat16)
        for slot in range(EPG):
            part_g[d, slot] = packed[:, slot * packed_width : (slot + 1) * packed_width]
        s["pg"] = copies.start(part_g.at[d, pl.ds(2, 2)], rc_g.at[d], ec)
        shares = 2 if d == groups - 1 else 1
        kept = EPG // shares

        def rows_back(lo, hi, half):
            part = slice(half * rows // shares, (half + 1) * rows // shares)
            total = lax.dot_general(
                grad_gate[part], first[lo:hi, :], CONTRACT_COLS, preferred_element_type=jnp.float32
            ) + lax.dot_general(
                grad_up[part], second[lo:hi, :], CONTRACT_COLS, preferred_element_type=jnp.float32
            )
            return total.astype(jnp.bfloat16).reshape(kept, cap, hi - lo)

        for half in reversed(range(shares)):
            slots = slice(half * kept, (half + 1) * kept)
            for lane in range(lanes):
                lo = lane * piece
                part_a[d, lane, slots] = rows_back(lo, lo + wide0, half)
            if half == shares - 1:
                s["pa"] = copies.start(part_a.at[d, :, pl.ds(2, 2)], rc_a.at[d], ec)
            for lane in range(lanes):
                lo = lane * piece
                if wide1:
                    part_b[d, lane, slots] = rows_back(lo + wide0, lo + piece, half)
            if half == shares - 1 and wide1:
                s["pb"] = copies.start(part_b.at[d, :, pl.ds(2, 2)], rc_b.at[d], ec)

    def sum_cores(d):
        s = state[d]
        s["pa"].wait_recv()
        s1_a[d] = add(part_a[d, :, 0:2], rc_a[d])
        s["x0"] = copies.start(s1_a.at[d, :, 1], rx_a.at[d], ex)
        s["pg"].wait_recv()
        s1_g[d] = add(part_g[d, 0:2], rc_g[d])
        s["xg"] = copies.start(s1_g.at[d, 1], rx_g.at[d], ex)
        if wide1:
            s["pb"].wait_recv()
            s1_b[d] = add(part_b[d, :, 0:2], rc_b[d])
            s["l1"] = [
                copies.start(s1_b.at[d, lane], rl_b.at[d, i], (g, e, lane))
                for i, lane in enumerate(ahead)
            ]

    def middle_sum(d):
        s = state[d]
        s["x0"].wait_recv()
        s2_a[d] = add(s1_a[d, :, 0], rx_a[d])
        s["l0"] = [
            copies.start(s2_a.at[d, lane], rl_a.at[d, i], (g, e, lane))
            for i, lane in enumerate(ahead)
        ]
        s["xg"].wait_recv()
        s2_g[d] = add(s1_g[d, 0], rx_g[d])
        s["lg"] = [
            copies.start(s2_g.at[d], rl_g.at[d, i], (g, e, lane)) for i, lane in enumerate(ahead)
        ]
        if wide1:
            for copy in s["l1"]:
                copy.wait_recv()
            s2_b[d] = add(s1_b[d, y], *[rl_b[d, i] for i in range(lanes - 1)])
            s["x1"] = copies.start(s2_b.at[d, 1], rx_b.at[d], ex)

    def last_sum(d):
        s = state[d]
        rows_at, gates_at, at = (ret, ret_g, g) if d == 0 else (done, done_g, d)
        for copy in s["l0"]:
            copy.wait_recv()
        there = (partner(g, d, groups, 1), e, y)
        s["z"] = []

        def home(*pieces):
            if d:
                s["z"] += [copies.start(src, dst, there) for src, dst in pieces]

        head, tail = pl.ds(0, wide0), pl.ds(wide0, wide1)
        rows_at[at, :, :wide0] = add(s2_a[d, y], *[rl_a[d, i] for i in range(lanes - 1)])
        home((done.at[d, :, head], ret.at[g, :, head]))
        for copy in s["lg"]:
            copy.wait_recv()
        gates_at[at] = add(s2_g[d], *[rl_g[d, i] for i in range(lanes - 1)])
        if wide1:
            s["x1"].wait_recv()
            rows_at[at, :, wide0:] = add(s2_b[d, 0], rx_b[d])
            home((done.at[d, :, tail], ret.at[g, :, tail]))
        home((done_g.at[d], ret_g.at[g]))

    tile = min(2 * LANES, piece)
    per = piece // tile
    tiles = feature_count // tile
    seen = [0]

    def weights_to(end):
        if seen[0] == 0 and end > 0:
            wt_t[...] = wt[...].T
        grads_gate, grads_up = gg[...], gu[...]
        left = wt_t[...]

        def turn(i, carry):
            lane, cols = i // per, pl.ds(pl.multiple_of(lax.rem(i, per) * tile, LANES), tile)
            turned = tok[lane, :, :, :, cols].reshape(groups * rows, tile).T
            at = pl.ds(pl.multiple_of(i * tile, LANES), tile)
            grad_first[at, :] = dot(turned, grads_gate)
            grad_second[at, :] = dot(turned, grads_up)
            grad_third[:, at] = dot(left, cot[lane, :, :, :, cols].reshape(groups * rows, tile))
            return carry

        if end > seen[0]:
            lax.fori_loop(seen[0], end, turn, 0)
        seen[0] = end

    steps = plan(groups)
    shares = sum(name == "weights" for name, _ in steps)
    served = [0]

    def weights(_):
        served[0] += 1
        weights_to(tiles * served[0] // shares)

    phases = {
        "own": own, "arrive_t": arrive_t, "arrive_c": arrive_c, "relay_t": relay_t,
        "relay_c": relay_c, "inside_t": inside_t, "inside_z": inside_z, "inside_c": inside_c, "compute": compute, "compute_t": compute_t,
        "sum_cores": sum_cores, "middle_sum": middle_sum, "last_sum": last_sum,
        "weights": weights, "next_t": next_t, "next_c": next_c, "rest_t": rest_t, "rest_c": rest_c,
    }
    for name, d in steps:
        with jax.named_scope(f"{name}_{d}"):
            phases[name](d)
    with jax.named_scope("gather"):
        for d in range(1, groups):
            for copy in state[d]["z"]:
                copy.wait_recv()
        token_grad[...] = lax.dot_general(
            one_hot, ret[...].reshape(groups * cap, piece), CONTRACT_ROWS,
            preferred_element_type=jnp.float32,
        )
        total = dot(ret_g[0, :, :cap], pick[0])
        for group in range(1, groups):
            total = total + dot(ret_g[group, :, :cap], pick[group])
        gate_grad[...] = total
    with jax.named_scope("finish"):
        copies.finish()


def route(choice, weight, weights_t, local_t, tokens, cotangent, w_gate, w_up, w_down, groups, lanes, cap):
    token_count, feature_count = tokens.shape
    hidden_count = w_gate.shape[1]
    piece = feature_count // lanes
    wide1 = piece // (2 * LANES) * LANES
    wide0 = piece - wide1
    tail = max(wide1, LANES)
    packed = -(-cap // LANES) * LANES
    rows = EPG * cap
    far = max(lanes - 1, 1)
    count = copy_count(groups, lanes)
    vmem, hbm = pl.BlockSpec(memory_space=pltpu.VMEM), pl.BlockSpec(memory_space=pltpu.HBM)

    def buffer(*shape):
        return pltpu.VMEM(shape, jnp.bfloat16)

    def grad(*shape):
        return jax.ShapeDtypeStruct(shape, jnp.float32)

    return pl.pallas_call(
        functools.partial(kernel, groups, lanes, cap, wide0, wide1),
        out_shape=(
            grad(token_count, piece),
            grad(PACKED, token_count),
            grad(feature_count, hidden_count),
            grad(feature_count, hidden_count),
            grad(hidden_count, feature_count),
        ),
        in_specs=[hbm] * 9,
        out_specs=(vmem,) * 5,
        scratch_shapes=[
            pltpu.VMEM(choice.shape, choice.dtype),
            pltpu.VMEM(weight.shape, weight.dtype),
            pltpu.VMEM(weights_t.shape, weights_t.dtype),
            pltpu.VMEM(local_t.shape, local_t.dtype),
            buffer(token_count, feature_count),
            buffer(token_count, feature_count),
            buffer(groups, cap, token_count),
            buffer(groups, cap, piece),
            buffer(groups, cap, piece),
            buffer(groups, PACKED, packed),
            buffer(2, lanes, cap, piece),
            buffer(2, lanes, cap, piece),
            buffer(lanes, groups, EPG, cap, piece),
            buffer(lanes, groups, EPG, cap, piece),
            buffer(groups, EPG, PACKED, packed),
            buffer(feature_count, hidden_count),
            buffer(feature_count, hidden_count),
            buffer(hidden_count, feature_count),
            pltpu.VMEM((2, rows, hidden_count), jnp.float32),
            buffer(groups * rows, hidden_count),
            buffer(groups * rows, hidden_count),
            buffer(groups * rows, hidden_count),
            buffer(hidden_count, groups * rows),
            buffer(groups, lanes, EPG, cap, wide0),
            buffer(groups, lanes, EPG, cap, tail),
            buffer(groups, lanes, 2, cap, wide0),
            buffer(groups, lanes, 2, cap, tail),
            buffer(groups, lanes, 2, cap, wide0),
            buffer(groups, lanes, 2, cap, tail),
            buffer(groups, lanes, cap, wide0),
            buffer(groups, far, cap, wide0),
            buffer(groups, far, 2, cap, tail),
            buffer(groups, lanes, cap, wide0),
            buffer(groups, 2, cap, tail),
            buffer(groups, cap, tail),
            buffer(groups, cap, piece),
            buffer(groups, cap, piece),
            buffer(groups, EPG, PACKED, packed),
            buffer(groups, 2, PACKED, packed),
            buffer(groups, 2, PACKED, packed),
            buffer(groups, PACKED, packed),
            buffer(groups, PACKED, packed),
            buffer(groups, far, PACKED, packed),
            buffer(groups, PACKED, packed),
            buffer(groups, PACKED, packed),
            pltpu.SemaphoreType.DMA((SENDS + 3 * max(groups - 1, 1),)),
            pltpu.SemaphoreType.DMA((count,)),
            pltpu.SemaphoreType.DMA((9,)),
        ],
        compiler_params=pltpu.CompilerParams(
            collective_id=0, has_side_effects=True, vmem_limit_bytes=VMEM_LIMIT
        ),
        name="routed_backward",
    )(choice, weight, weights_t, local_t, tokens, cotangent, w_gate, w_up, w_down)


def finish_kernel(
    weight, weights_t, local_t, gate_grad, token_grad, first, second, third,
    group_out, expert_out, token_out, first_out, second_out, third_out, sem,
):
    parts = [
        (src.at[pl.ds(i * src.shape[0] // PARTS, src.shape[0] // PARTS)],
         dst.at[pl.ds(i * src.shape[0] // PARTS, src.shape[0] // PARTS)])
        for i in range(PARTS)
        for src, dst in (
            (first, first_out), (second, second_out), (third, third_out), (token_grad, token_out)
        )
    ]
    moves = [
        pltpu.make_async_copy(src, dst, sem.at[i]) for i, (src, dst) in enumerate(parts)
    ]
    for move in moves:
        move.start()
    total = None
    for k in range(local_t.shape[0]):
        hit = lax.broadcasted_iota(jnp.int32, gate_grad.shape, 0) == local_t[k : k + 1, :]
        held = jnp.sum(jnp.where(hit, gate_grad[...], 0.0), axis=0, keepdims=True)
        held = held.astype(jnp.bfloat16).astype(jnp.float32)
        expert_out[k : k + 1, :] = weight[...] * held
        term = weights_t[k : k + 1, :] * held
        total = term if total is None else total + term
    group_out[...] = total
    for move in moves:
        move.wait()


def finish(weight, weights_t, local_t, gate_grad, token_grad, first, second, third):
    vmem, hbm = pl.BlockSpec(memory_space=pltpu.VMEM), pl.BlockSpec(memory_space=pltpu.HBM)

    def like(array):
        return jax.ShapeDtypeStruct(array.shape, jnp.float32)

    return pl.pallas_call(
        finish_kernel,
        out_shape=(
            like(weight), like(weights_t), like(token_grad), like(first), like(second), like(third)
        ),
        in_specs=[vmem] * 8,
        out_specs=(vmem,) * 2 + (hbm,) * 4,
        scratch_shapes=[pltpu.SemaphoreType.DMA((4 * PARTS,))],
        compiler_params=pltpu.CompilerParams(vmem_limit_bytes=FINISH_LIMIT),
        name="write_results",
    )(weight, weights_t, local_t, gate_grad, token_grad, first, second, third)


def shards(
    tokens, cotangent, group_weight, expert_weight, group_choice, local_choice, w_gate, w_up, w_down
):
    token_count = tokens.shape[0]
    pick_count = expert_weight.shape[1]
    group_count = lax.axis_size("g")
    lane_count = lax.axis_size("tp")
    expert_count = group_count * EPG
    capacity = pick_count * (3 * token_count // (2 * expert_count))
    group_cap = -(-(EPG * capacity // pick_count) // 16) * 16
    weight = group_weight.reshape(1, token_count)
    weights_t, local_t = expert_weight.T, local_choice.T
    operands = (
        group_choice.reshape(1, token_count), weight, weights_t, local_t,
        tokens, cotangent, w_gate[0], w_up[0], w_down[0],
    )
    operands = [pltpu.with_memory_space_constraint(array, pltpu.HBM) for array in operands]
    token_grad, gate_grad, first_grad, second_grad, third_grad = route(
        *operands, group_count, lane_count, group_cap
    )
    group_grad, expert_grad, token_grad, first_grad, second_grad, third_grad = finish(
        weight, weights_t, local_t, gate_grad, token_grad, first_grad, second_grad, third_grad
    )
    return (
        token_grad,
        group_grad.reshape(token_count),
        expert_grad.T,
        first_grad[None],
        second_grad[None],
        third_grad[None],
    )


def solution(mesh):
    lanes = mesh.shape["tp"]
    split = Mesh(mesh.devices.reshape(-1, EPG, lanes), ("g", "e", "tp"))
    ep = ("g", "e")
    in_specs = (
        P(ep, None),
        P(ep, None),
        P(ep),
        P(ep, None),
        P(ep),
        P(ep, None),
        P(ep, None, "tp"),
        P(ep, None, "tp"),
        P(ep, "tp", None),
    )
    out_specs = (
        P(ep, "tp"),
        P(ep),
        P(ep, None),
        P(ep, None, "tp"),
        P(ep, None, "tp"),
        P(ep, "tp", None),
    )
    return jax.shard_map(
        shards, mesh=split, in_specs=in_specs, out_specs=out_specs, check_vma=False
    )
```

```python
import functools

import jax
import jax.numpy as jnp
from jax import lax
from jax.experimental import pallas as pl
from jax.experimental.pallas import tpu as pltpu
from jax.sharding import Mesh, PartitionSpec as P

EPG = 4
LANES = 128
PACKED = 16
SENDS = 20
PARTS = 1
VMEM_LIMIT = 36 * 1024 * 1024
FINISH_LIMIT = 16 * 1024 * 1024

MESH = pl.DeviceIdType.MESH

CONTRACT_COLS = (((1,), (1,)), ((), ()))
CONTRACT_ROWS = (((0,), (0,)), ((), ()))


def partner(g, d, groups, sign):
    if groups & (groups - 1):
        return lax.rem(g + sign * d + groups, groups)
    met, bit = g, 1
    while bit < groups:
        if d & bit:
            met = met + bit - 2 * bit * ((g // bit) % 2)
        bit *= 2
    return met


def is_inner(g, groups):
    return 0 if groups & (groups - 1) else (g + g // 2) % 2


class Copies:
    def __init__(self, send_sem, recv_sem):
        self.send_sem, self.recv_sem, self.count, self.made = send_sem, recv_sem, 0, []
        self.kept = []

    def describe(self, src, dst, device, number, slot):
        return pltpu.make_async_remote_copy(
            src_ref=src,
            dst_ref=dst,
            send_sem=self.send_sem.at[slot],
            recv_sem=self.recv_sem.at[number],
            device_id=device,
            device_id_type=MESH,
        )

    def reserve(self, count):
        self.count += count
        return self.count - count

    def start(self, src, dst, device, number=None):
        slot = len(self.made) % SENDS
        if len(self.made) >= SENDS:
            self.made[len(self.made) - SENDS].wait_send()
        number = self.reserve(1) if number is None else number
        copy = self.describe(src, dst, device, number, slot)
        copy.start()
        self.made.append(copy)
        return copy

    def finish(self):
        for copy in self.kept + self.made[-SENDS:]:
            copy.wait_send()


def whole_groups(groups, lanes):
    return range(1, min(groups, 2)) if lanes == 2 else range(0)


def copy_count(groups, lanes):
    far = lanes - 1
    whole = len(whole_groups(groups, lanes))
    first = (groups - 1) * 3 + whole * 2 * far
    spread = (groups - 1 - whole) * (2 + 4 * far) + (1 + whole) * (2 + 2 * far)
    inside = groups * 4
    back = groups * (6 + 3 * far) + 3 * (groups - 1)
    return first + spread + inside + back


def dot(a, b):
    return jnp.dot(a, b, preferred_element_type=jnp.float32)


def add(*parts):
    total = parts[0].astype(jnp.float32)
    for part in parts[1:]:
        total = total + part.astype(jnp.float32)
    return total.astype(jnp.bfloat16)


def plan(groups):
    steps = []

    def put(names, d):
        for name in names.split():
            if (0 <= d < groups or name == "weights") and (name, d) not in steps and (d or not name.startswith("arrive")):
                steps.append((name, d))

    put("own next_t relay_t", 0)
    put("arrive_t", 1)
    put("relay_c", 0)
    put("arrive_c relay_t", 1)
    put("next_c", 0)
    put("relay_c", 1)
    put("inside_t inside_c", 0)
    put("arrive_t", 2)
    put("rest_t compute", 0)
    put("inside_t inside_c", 1)
    put("arrive_c", 2)
    put("rest_c", 0)
    put("relay_t", 2)
    put("inside_z", 1)
    put("arrive_t", 3)
    put("relay_c", 2)
    for d in range(3, groups):
        put("arrive_t arrive_c", d)
        put("compute", d - 2)
        put("inside_t inside_c", d - 1)
        put("relay_t relay_c", d)
        put("sum_cores", d - 2)
        put("sum_cores", 0)
        put("compute", d - 1)
        if d < groups - 1:
            put("middle_sum last_sum", d - 2)
    last = groups - 1
    before = last - 1 if last > 2 else 0
    put("compute", 1)
    put("inside_t", last)
    if before:
        put("sum_cores", before)
    put("inside_c", last)
    if last > 1:
        put("compute_t", last)
    if before:
        put("middle_sum", before - 1)
    put("compute", last)
    if before:
        put("middle_sum", before)
    if last > 0:
        put("sum_cores", last)
    put("weights", 0)
    if before:
        put("last_sum", before - 1)
        put("middle_sum", 0)
    if before:
        put("last_sum", before)
    put("weights", 1)
    if last > 0:
        put("middle_sum", last)
    put("sum_cores", 0)
    if last == 2:
        put("sum_cores middle_sum last_sum", 1)
    put("weights", 2)
    if last > 0:
        put("last_sum", last)
    put("middle_sum last_sum", 0)
    put("weights", 3)
    return steps


def kernel(
    groups, lanes, cap, wide0, wide1,
    choice_in, weight_in, weights_in, local_in, tokens_in, cotangent_in, w_gate, w_up, w_down,
    token_grad, gate_grad, grad_first, grad_second, grad_third,
    choice, weight, weights_t, local_t, tokens, cotangent, pick, out_t, out_c, out_g, all_t, all_c, tok, cot, gate, first, second, third,
    pre, gg, gu, wt, wt_t, part_a, part_b, rc_a, rc_b, s1_a, s1_b, rx_a, rl_a, rl_b, s2_a, s2_b, rx_b,
    done, ret, part_g, rc_g, s1_g, rx_g, s2_g, rl_g, done_g, ret_g, send, recv, loc,
):
    g, e, y = lax.axis_index("g"), lax.axis_index("e"), lax.axis_index("tp")
    x, c = e // 2, e % 2
    ex, ec = (g, (1 - x) * 2 + c, y), (g, x * 2 + (1 - c), y)
    token_count, feature_count = tokens.shape
    piece = feature_count // lanes
    rows = EPG * cap
    far = range(1, lanes)
    ahead = [lax.rem(y + r, lanes) for r in far]
    behind = [lax.rem(y + lanes - r, lanes) for r in far]
    others = [(g, e, lane) for lane in ahead]

    loads = [
        pltpu.make_async_copy(src, dst, loc.at[i])
        for i, (src, dst) in enumerate(
            (
                (choice_in, choice), (weight_in, weight), (weights_in, weights_t),
                (local_in, local_t), (tokens_in, tokens), (cotangent_in, cotangent),
                (w_gate, first), (w_up, second), (w_down, third),
            )
        )
    ]
    for load in loads[:6]:
        load.start()
    barrier = pltpu.get_barrier_semaphore()
    met = [(lax.rem(g + d, groups), e, y) for d in range(1, groups)] + others + [ex, ec]
    for device in met:
        pl.semaphore_signal(barrier, inc=1, device_id=device, device_id_type=MESH)

    def iota(shape, dim):
        return lax.broadcasted_iota(jnp.int32, shape, dim)

    def spread_rows(rows_of, source):
        return dot(rows_of, source).astype(jnp.bfloat16)

    for load in loads[:4]:
        load.wait()
    chosen = choice[...]
    square = (token_count, token_count)
    earlier = (iota(square, 0) < iota(square, 1)).astype(jnp.float32).astype(jnp.bfloat16)
    high = -(-groups // 16) * 16
    named = iota((high, token_count), 0) == chosen
    member = jnp.where(named, 1.0, 0.0)
    rank = jnp.sum(member * dot(member.astype(jnp.bfloat16), earlier), axis=0, keepdims=True)
    rank = jnp.where(rank < cap, rank, cap).astype(jnp.int32)
    dest = chosen * cap + rank
    one_hot = jnp.where(iota((groups * cap, token_count), 0) == dest, 1.0, 0.0).astype(jnp.bfloat16)
    pick[...] = one_hot.reshape(groups, cap, token_count)
    gates = (weight[...] * weights_t[...]).astype(jnp.bfloat16).astype(jnp.float32)
    gate_rows = jnp.zeros((PACKED, token_count), jnp.float32)
    for k in range(local_t.shape[0]):
        hit = iota((PACKED, token_count), 0) == local_t[k : k + 1, :]
        gate_rows = gate_rows + jnp.where(hit, gates[k : k + 1, :], 0.0)
    columns = pl.ds(pl.multiple_of(y * piece, LANES), piece)
    packed_width = out_g.shape[2]
    wide_dest = chosen * packed_width + rank
    wide_hot = iota((groups * packed_width, token_count), 0) == wide_dest
    blocks = lax.dot_general(
        gate_rows.astype(jnp.bfloat16),
        jnp.where(wide_hot, 1.0, 0.0).astype(jnp.bfloat16),
        CONTRACT_COLS,
        preferred_element_type=jnp.float32,
    ).astype(jnp.bfloat16)
    for group in range(groups):
        out_g[group] = blocks[:, group * packed_width : (group + 1) * packed_width]
    loads[4].wait()
    out_t[...] = spread_rows(one_hot, tokens[:, columns]).reshape(groups, cap, piece)
    loads[5].wait()
    out_c[...] = spread_rows(one_hot, cotangent[:, columns]).reshape(groups, cap, piece)
    whole = whole_groups(groups, lanes)
    pl.semaphore_wait(barrier, len(met))

    copies = Copies(send, recv)
    state = [dict() for _ in range(groups)]
    base = copies.reserve(3 * (groups - 1))

    def cross(d, target):
        there = (target, e, y)
        number = base + 3 * (d - 1)
        return [
            copies.describe(out_t.at[target], tok.at[y, d, 0], there, number, SENDS + number),
            copies.describe(out_g.at[target], gate.at[d, 0], there, number + 1, SENDS + number + 1),
            copies.describe(out_c.at[target], cot.at[y, d, 0], there, number + 2, SENDS + number + 2),
        ]

    def send(ds, kinds):
        for d in ds:
            for kind in kinds:
                cross(d, partner(g, d, groups, -1))[kind].start()

    inner = is_inner(g, groups)
    far_first = groups > 3 and not isinstance(inner, int)
    send(range(1, min(groups, 2)), (0, 1, 2))
    if far_first:
        pl.when(inner == 1)(lambda: send([3], (0, 1, 2)))
    for load in loads[6:]:
        load.start()

    def fill_whole():
        for d in whole:
            mine = pick[partner(g, d, groups, -1)]
            for lane in ahead:
                cols = pl.ds(pl.multiple_of(lane * piece, LANES), piece)
                all_t[d, lane] = spread_rows(mine, tokens[:, cols])
                all_c[d, lane] = spread_rows(mine, cotangent[:, cols])

    def send_whole(source, target, name):
        for d in whole:
            there = (partner(g, d, groups, -1), e, y)
            state[d][name] = [
                copies.start(source.at[d, lane], target.at[lane, d, 0], there) for lane in ahead
            ]

    def next_t(_):
        send(range(2, min(groups, 3)), (0, 1))
        send_whole(all_t, tok, "zat")

    def next_c(_):
        send(range(2, min(groups, 3)), (2,))
        send_whole(all_c, cot, "zac")

    def rest(kinds):
        if far_first:
            pl.when(inner == 0)(lambda: send([3], kinds))
        send(range(4 if far_first else 3, groups), kinds)

    def rest_t(_):
        rest((0, 1))

    def rest_c(_):
        rest((2,))

    for d in range(1, groups):
        arriving = cross(d, partner(g, d, groups, -1))
        copies.kept += arriving
        state[d]["zt"], state[d]["zg"], state[d]["zc"] = arriving

    inner_base = copies.reserve(3 * groups)

    def to_core(d, kind, slot):
        ref = (tok, gate, cot)[kind]
        if kind == 1:
            src, dst = gate.at[d, slot], gate.at[d, slot + 2]
        else:
            src, dst = ref.at[:, d, slot], ref.at[:, d, slot + 2]
        copies.start(src, dst, ec, inner_base + 3 * d + kind)

    def wait_core(d, kinds):
        for kind in kinds:
            ref = (tok, gate, cot)[kind]
            if kind == 1:
                src, dst = gate.at[d, pl.ds(0, 2)], gate.at[d, pl.ds(2, 2)]
            else:
                src, dst = ref.at[:, d, pl.ds(0, 2)], ref.at[:, d, pl.ds(2, 2)]
            copies.describe(src, dst, ec, inner_base + 3 * d + kind, 0).wait_recv()

    def own(_):
        s = state[0]
        s["tx"] = [copies.start(out_t.at[g], tok.at[y, 0, 1], ex)]
        s["gx"] = copies.start(out_g.at[g], gate.at[0, 1], ex)
        s["cx"] = copies.start(out_c.at[g], cot.at[y, 0, 1], ex)
        mine = pick[g]
        for lane in range(lanes):
            cols = slice(lane * piece, (lane + 1) * piece)
            tok[lane, 0, 0] = spread_rows(mine, tokens[:, cols])
            cot[lane, 0, 0] = spread_rows(mine, cotangent[:, cols])
        gate[0, 0] = out_g[g]
        for kind in (1, 0, 2):
            to_core(0, kind, 0)
        fill_whole()

    def arrive_t(d):
        s = state[d]
        s["zt"].wait_recv()
        mine = tok.at[y, d, 0]
        if d not in whole:
            s["tl"] = [copies.start(mine, mine, device) for device in others]
        s["tx"] = [copies.start(mine, tok.at[y, d, 1], ex)]
        s["zg"].wait_recv()
        s["gx"] = copies.start(gate.at[d, 0], gate.at[d, 1], ex)
        to_core(d, 1, 0)

    def arrive_c(d):
        s = state[d]
        s["zc"].wait_recv()
        mine = cot.at[y, d, 0]
        s["cx"] = copies.start(mine, cot.at[y, d, 1], ex)
        if d not in whole:
            s["cl"] = [copies.start(mine, mine, device) for device in others]

    def relay_t(d):
        s = state[d]
        if d == 0 or d in whole:
            s["tx"][0].wait_recv()
            theirs = tok.at[y, d, 1]
            s["txl"] = [copies.start(theirs, theirs, device) for device in others]
        else:
            for i, copy in enumerate(s["tl"]):
                copy.wait_recv()
                theirs = tok.at[behind[i], d, 0]
                s["tx"].append(copies.start(theirs, tok.at[behind[i], d, 1], ex))
            to_core(d, 0, 0)

    def relay_c(d):
        s = state[d]
        s["cx"].wait_recv()
        theirs = cot.at[y, d, 1]
        s["cxl"] = [copies.start(theirs, theirs, device) for device in others]

    def inside_z(d):
        s = state[d]
        if d in whole:
            for copy in s["zat"]:
                copy.wait_recv()
            to_core(d, 0, 0)
            for copy in s["zac"]:
                copy.wait_recv()
            to_core(d, 2, 0)

    def inside_t(d):
        s = state[d]
        if d == 0 or d in whole:
            for copy in s["txl"]:
                copy.wait_recv()
        else:
            for copy in s["cl"]:
                copy.wait_recv()
            to_core(d, 2, 0)
            for copy in s["tx"]:
                copy.wait_recv()
        to_core(d, 0, 1)

    def inside_c(d):
        s = state[d]
        s["gx"].wait_recv()
        to_core(d, 1, 1)
        for copy in s["cxl"]:
            copy.wait_recv()
        to_core(d, 2, 1)

    loaded = []

    begun = set()

    def compute_t(d):
        begun.add(d)
        if not loaded:
            for load in loads[6:]:
                load.wait()
            loaded.append(True)
        wait_core(d, (0,))
        for half, weights_in in enumerate((first, second)):
            total = None
            for lane in range(lanes):
                cols = slice(lane * piece, (lane + 1) * piece)
                term = dot(tok[lane, d].reshape(rows, piece), weights_in[cols, :])
                total = term if total is None else total + term
            pre[half] = total

    def compute(d):
        s = state[d]
        if d not in begun:
            compute_t(d)
        wait_core(d, (1, 2))
        back = None
        for lane in range(lanes):
            cols = slice(lane * piece, (lane + 1) * piece)
            term = lax.dot_general(
                cot[lane, d].reshape(rows, piece), third[:, cols], CONTRACT_COLS,
                preferred_element_type=jnp.float32,
            )
            back = term if back is None else back + term
        pre_gate, pre_up = pre[0], pre[1]
        own_col = iota((rows, LANES), 1) == e
        own_row = jnp.where(iota((PACKED, LANES), 0) == e, 1.0, 0.0).astype(jnp.bfloat16)
        gate_float = jnp.concatenate(
            [
                lax.dot_general(
                    gate[d, slot, :, :cap], own_row, CONTRACT_ROWS, preferred_element_type=jnp.float32
                )
                for slot in range(EPG)
            ],
            axis=0,
        )[:, :1]
        sigma = jax.nn.sigmoid(pre_gate)
        swish = pre_gate * sigma
        hidden = swish * pre_up
        gate_part = jnp.sum(hidden * back, axis=1, keepdims=True)
        scaled = gate_float * back
        grad_gate = (scaled * pre_up * sigma * (1.0 + pre_gate * (1.0 - sigma))).astype(jnp.bfloat16)
        grad_up = (scaled * swish).astype(jnp.bfloat16)
        at = slice(d * rows, (d + 1) * rows)
        gg[at, :] = grad_gate
        gu[at, :] = grad_up
        wt[at, :] = (gate_float * hidden).astype(jnp.bfloat16)
        gate_out = jnp.where(own_col, gate_part, 0.0).astype(jnp.bfloat16)

        blocks = gate_out.reshape(EPG, cap, LANES)
        if packed_width > cap:
            filler = jnp.zeros((EPG, packed_width - cap, LANES), jnp.bfloat16)
            blocks = jnp.concatenate([blocks, filler], axis=1)
        chooser = jnp.where(iota((PACKED, LANES), 0) == iota((PACKED, LANES), 1), 1.0, 0.0)
        packed = lax.dot_general(
            chooser.astype(jnp.bfloat16),
            blocks.reshape(EPG * packed_width, LANES),
            CONTRACT_COLS,
            preferred_element_type=jnp.float32,
        ).astype(jnp.bfloat16)
        for slot in range(EPG):
            part_g[d, slot] = packed[:, slot * packed_width : (slot + 1) * packed_width]
        s["pg"] = copies.start(part_g.at[d, pl.ds(2, 2)], rc_g.at[d], ec)
        shares = 2 if d == groups - 1 else 1
        kept = EPG // shares

        def rows_back(lo, hi, half):
            part = slice(half * rows // shares, (half + 1) * rows // shares)
            total = lax.dot_general(
                grad_gate[part], first[lo:hi, :], CONTRACT_COLS, preferred_element_type=jnp.float32
            ) + lax.dot_general(
                grad_up[part], second[lo:hi, :], CONTRACT_COLS, preferred_element_type=jnp.float32
            )
            return total.astype(jnp.bfloat16).reshape(kept, cap, hi - lo)

        for half in reversed(range(shares)):
            slots = slice(half * kept, (half + 1) * kept)
            for lane in range(lanes):
                lo = lane * piece
                part_a[d, lane, slots] = rows_back(lo, lo + wide0, half)
            if half == shares - 1:
                s["pa"] = copies.start(part_a.at[d, :, pl.ds(2, 2)], rc_a.at[d], ec)
            for lane in range(lanes):
                lo = lane * piece
                if wide1:
                    part_b[d, lane, slots] = rows_back(lo + wide0, lo + piece, half)
            if half == shares - 1 and wide1:
                s["pb"] = copies.start(part_b.at[d, :, pl.ds(2, 2)], rc_b.at[d], ec)

    def sum_cores(d):
        s = state[d]
        s["pa"].wait_recv()
        s1_a[d] = add(part_a[d, :, 0:2], rc_a[d])
        s["x0"] = copies.start(s1_a.at[d, :, 1], rx_a.at[d], ex)
        s["pg"].wait_recv()
        s1_g[d] = add(part_g[d, 0:2], rc_g[d])
        s["xg"] = copies.start(s1_g.at[d, 1], rx_g.at[d], ex)
        if wide1:
            s["pb"].wait_recv()
            s1_b[d] = add(part_b[d, :, 0:2], rc_b[d])
            s["l1"] = [
                copies.start(s1_b.at[d, lane], rl_b.at[d, i], (g, e, lane))
                for i, lane in enumerate(ahead)
            ]

    def middle_sum(d):
        s = state[d]
        s["x0"].wait_recv()
        s2_a[d] = add(s1_a[d, :, 0], rx_a[d])
        s["l0"] = [
            copies.start(s2_a.at[d, lane], rl_a.at[d, i], (g, e, lane))
            for i, lane in enumerate(ahead)
        ]
        s["xg"].wait_recv()
        s2_g[d] = add(s1_g[d, 0], rx_g[d])
        s["lg"] = [
            copies.start(s2_g.at[d], rl_g.at[d, i], (g, e, lane)) for i, lane in enumerate(ahead)
        ]
        if wide1:
            for copy in s["l1"]:
                copy.wait_recv()
            s2_b[d] = add(s1_b[d, y], *[rl_b[d, i] for i in range(lanes - 1)])
            s["x1"] = copies.start(s2_b.at[d, 1], rx_b.at[d], ex)

    def last_sum(d):
        s = state[d]
        rows_at, gates_at, at = (ret, ret_g, g) if d == 0 else (done, done_g, d)
        for copy in s["l0"]:
            copy.wait_recv()
        there = (partner(g, d, groups, 1), e, y)
        s["z"] = []

        def home(*pieces):
            if d:
                s["z"] += [copies.start(src, dst, there) for src, dst in pieces]

        head, tail = pl.ds(0, wide0), pl.ds(wide0, wide1)
        rows_at[at, :, :wide0] = add(s2_a[d, y], *[rl_a[d, i] for i in range(lanes - 1)])
        home((done.at[d, :, head], ret.at[g, :, head]))
        for copy in s["lg"]:
            copy.wait_recv()
        gates_at[at] = add(s2_g[d], *[rl_g[d, i] for i in range(lanes - 1)])
        if wide1:
            s["x1"].wait_recv()
            rows_at[at, :, wide0:] = add(s2_b[d, 0], rx_b[d])
            home((done.at[d, :, tail], ret.at[g, :, tail]))
        home((done_g.at[d], ret_g.at[g]))

    tile = min(2 * LANES, piece)
    per = piece // tile
    tiles = feature_count // tile
    seen = [0]

    def weights_to(end):
        if seen[0] == 0 and end > 0:
            wt_t[...] = wt[...].T
        grads_gate, grads_up = gg[...], gu[...]
        left = wt_t[...]

        def turn(i, carry):
            lane, cols = i // per, pl.ds(pl.multiple_of(lax.rem(i, per) * tile, LANES), tile)
            turned = tok[lane, :, :, :, cols].reshape(groups * rows, tile).T
            at = pl.ds(pl.multiple_of(i * tile, LANES), tile)
            grad_first[at, :] = dot(turned, grads_gate)
            grad_second[at, :] = dot(turned, grads_up)
            grad_third[:, at] = dot(left, cot[lane, :, :, :, cols].reshape(groups * rows, tile))
            return carry

        if end > seen[0]:
            lax.fori_loop(seen[0], end, turn, 0)
        seen[0] = end

    steps = plan(groups)
    shares = sum(name == "weights" for name, _ in steps)
    served = [0]

    def weights(_):
        served[0] += 1
        weights_to(tiles * served[0] // shares)

    phases = {
        "own": own, "arrive_t": arrive_t, "arrive_c": arrive_c, "relay_t": relay_t,
        "relay_c": relay_c, "inside_t": inside_t, "inside_z": inside_z, "inside_c": inside_c, "compute": compute, "compute_t": compute_t,
        "sum_cores": sum_cores, "middle_sum": middle_sum, "last_sum": last_sum,
        "weights": weights, "next_t": next_t, "next_c": next_c, "rest_t": rest_t, "rest_c": rest_c,
    }
    for name, d in steps:
        with jax.named_scope(f"{name}_{d}"):
            phases[name](d)
    with jax.named_scope("gather"):
        for d in range(1, groups):
            for copy in state[d]["z"]:
                copy.wait_recv()
        token_grad[...] = lax.dot_general(
            one_hot, ret[...].reshape(groups * cap, piece), CONTRACT_ROWS,
            preferred_element_type=jnp.float32,
        )
        total = dot(ret_g[0, :, :cap], pick[0])
        for group in range(1, groups):
            total = total + dot(ret_g[group, :, :cap], pick[group])
        gate_grad[...] = total
    with jax.named_scope("finish"):
        copies.finish()


def route(choice, weight, weights_t, local_t, tokens, cotangent, w_gate, w_up, w_down, groups, lanes, cap):
    token_count, feature_count = tokens.shape
    hidden_count = w_gate.shape[1]
    piece = feature_count // lanes
    wide1 = piece // (2 * LANES) * LANES
    wide0 = piece - wide1
    tail = max(wide1, LANES)
    packed = -(-cap // LANES) * LANES
    rows = EPG * cap
    far = max(lanes - 1, 1)
    count = copy_count(groups, lanes)
    vmem, hbm = pl.BlockSpec(memory_space=pltpu.VMEM), pl.BlockSpec(memory_space=pltpu.HBM)

    def buffer(*shape):
        return pltpu.VMEM(shape, jnp.bfloat16)

    def grad(*shape):
        return jax.ShapeDtypeStruct(shape, jnp.float32)

    return pl.pallas_call(
        functools.partial(kernel, groups, lanes, cap, wide0, wide1),
        out_shape=(
            grad(token_count, piece),
            grad(PACKED, token_count),
            grad(feature_count, hidden_count),
            grad(feature_count, hidden_count),
            grad(hidden_count, feature_count),
        ),
        in_specs=[hbm] * 9,
        out_specs=(vmem,) * 5,
        scratch_shapes=[
            pltpu.VMEM(choice.shape, choice.dtype),
            pltpu.VMEM(weight.shape, weight.dtype),
            pltpu.VMEM(weights_t.shape, weights_t.dtype),
            pltpu.VMEM(local_t.shape, local_t.dtype),
            buffer(token_count, feature_count),
            buffer(token_count, feature_count),
            buffer(groups, cap, token_count),
            buffer(groups, cap, piece),
            buffer(groups, cap, piece),
            buffer(groups, PACKED, packed),
            buffer(2, lanes, cap, piece),
            buffer(2, lanes, cap, piece),
            buffer(lanes, groups, EPG, cap, piece),
            buffer(lanes, groups, EPG, cap, piece),
            buffer(groups, EPG, PACKED, packed),
            buffer(feature_count, hidden_count),
            buffer(feature_count, hidden_count),
            buffer(hidden_count, feature_count),
            pltpu.VMEM((2, rows, hidden_count), jnp.float32),
            buffer(groups * rows, hidden_count),
            buffer(groups * rows, hidden_count),
            buffer(groups * rows, hidden_count),
            buffer(hidden_count, groups * rows),
            buffer(groups, lanes, EPG, cap, wide0),
            buffer(groups, lanes, EPG, cap, tail),
            buffer(groups, lanes, 2, cap, wide0),
            buffer(groups, lanes, 2, cap, tail),
            buffer(groups, lanes, 2, cap, wide0),
            buffer(groups, lanes, 2, cap, tail),
            buffer(groups, lanes, cap, wide0),
            buffer(groups, far, cap, wide0),
            buffer(groups, far, 2, cap, tail),
            buffer(groups, lanes, cap, wide0),
            buffer(groups, 2, cap, tail),
            buffer(groups, cap, tail),
            buffer(groups, cap, piece),
            buffer(groups, cap, piece),
            buffer(groups, EPG, PACKED, packed),
            buffer(groups, 2, PACKED, packed),
            buffer(groups, 2, PACKED, packed),
            buffer(groups, PACKED, packed),
            buffer(groups, PACKED, packed),
            buffer(groups, far, PACKED, packed),
            buffer(groups, PACKED, packed),
            buffer(groups, PACKED, packed),
            pltpu.SemaphoreType.DMA((SENDS + 3 * max(groups - 1, 1),)),
            pltpu.SemaphoreType.DMA((count,)),
            pltpu.SemaphoreType.DMA((9,)),
        ],
        compiler_params=pltpu.CompilerParams(
            collective_id=0, has_side_effects=True, vmem_limit_bytes=VMEM_LIMIT
        ),
        name="routed_backward",
    )(choice, weight, weights_t, local_t, tokens, cotangent, w_gate, w_up, w_down)


def finish_kernel(
    weight, weights_t, local_t, gate_grad, token_grad, first, second, third,
    group_out, expert_out, token_out, first_out, second_out, third_out, sem,
):
    parts = [
        (src.at[pl.ds(i * src.shape[0] // PARTS, src.shape[0] // PARTS)],
         dst.at[pl.ds(i * src.shape[0] // PARTS, src.shape[0] // PARTS)])
        for i in range(PARTS)
        for src, dst in (
            (first, first_out), (second, second_out), (third, third_out), (token_grad, token_out)
        )
    ]
    moves = [
        pltpu.make_async_copy(src, dst, sem.at[i]) for i, (src, dst) in enumerate(parts)
    ]
    for move in moves:
        move.start()
    total = None
    for k in range(local_t.shape[0]):
        hit = lax.broadcasted_iota(jnp.int32, gate_grad.shape, 0) == local_t[k : k + 1, :]
        held = jnp.sum(jnp.where(hit, gate_grad[...], 0.0), axis=0, keepdims=True)
        held = held.astype(jnp.bfloat16).astype(jnp.float32)
        expert_out[k : k + 1, :] = weight[...] * held
        term = weights_t[k : k + 1, :] * held
        total = term if total is None else total + term
    group_out[...] = total
    for move in moves:
        move.wait()


def finish(weight, weights_t, local_t, gate_grad, token_grad, first, second, third):
    vmem, hbm = pl.BlockSpec(memory_space=pltpu.VMEM), pl.BlockSpec(memory_space=pltpu.HBM)

    def like(array):
        return jax.ShapeDtypeStruct(array.shape, jnp.float32)

    return pl.pallas_call(
        finish_kernel,
        out_shape=(
            like(weight), like(weights_t), like(token_grad), like(first), like(second), like(third)
        ),
        in_specs=[vmem] * 8,
        out_specs=(vmem,) * 2 + (hbm,) * 4,
        scratch_shapes=[pltpu.SemaphoreType.DMA((4 * PARTS,))],
        compiler_params=pltpu.CompilerParams(vmem_limit_bytes=FINISH_LIMIT),
        name="write_results",
    )(weight, weights_t, local_t, gate_grad, token_grad, first, second, third)


def shards(
    tokens, cotangent, group_weight, expert_weight, group_choice, local_choice, w_gate, w_up, w_down
):
    token_count = tokens.shape[0]
    pick_count = expert_weight.shape[1]
    group_count = lax.axis_size("g")
    lane_count = lax.axis_size("tp")
    expert_count = group_count * EPG
    capacity = pick_count * (3 * token_count // (2 * expert_count))
    group_cap = -(-(EPG * capacity // pick_count) // 16) * 16
    weight = group_weight.reshape(1, token_count)
    weights_t, local_t = expert_weight.T, local_choice.T
    operands = (
        group_choice.reshape(1, token_count), weight, weights_t, local_t,
        tokens, cotangent, w_gate[0], w_up[0], w_down[0],
    )
    operands = [pltpu.with_memory_space_constraint(array, pltpu.HBM) for array in operands]
    token_grad, gate_grad, first_grad, second_grad, third_grad = route(
        *operands, group_count, lane_count, group_cap
    )
    group_grad, expert_grad, token_grad, first_grad, second_grad, third_grad = finish(
        weight, weights_t, local_t, gate_grad, token_grad, first_grad, second_grad, third_grad
    )
    return (
        token_grad,
        group_grad.reshape(token_count),
        expert_grad.T,
        first_grad[None],
        second_grad[None],
        third_grad[None],
    )


def solution(mesh):
    lanes = mesh.shape["tp"]
    split = Mesh(mesh.devices.reshape(-1, EPG, lanes), ("g", "e", "tp"))
    ep = ("g", "e")
    in_specs = (
        P(ep, None),
        P(ep, None),
        P(ep),
        P(ep, None),
        P(ep),
        P(ep, None),
        P(ep, None, "tp"),
        P(ep, None, "tp"),
        P(ep, "tp", None),
    )
    out_specs = (
        P(ep, "tp"),
        P(ep),
        P(ep, None),
        P(ep, None, "tp"),
        P(ep, None, "tp"),
        P(ep, "tp", None),
    )
    return jax.shard_map(
        shards, mesh=split, in_specs=in_specs, out_specs=out_specs, check_vma=False
    )
```
